32 devices in a mesh: ep: 8 (over z, y), tp: 4 (over x, core).
Axes of the slice: x: 2, y: 2, z: 4, core: 2. Of those that a mesh axis runs over, the one named last changes fastest.
Arguments:
- mix_tokens: bfloat16 [8192, 2048], P(('ep', 'tp')), may hold values from -6 to 6
- mix_gain: bfloat16 [2048], replicated, may hold values from 0.099609375 to 1.8984375
- w_branch: bfloat16 [2048, 2048], P(None, 'tp'), may hold values from -0.125 to 0.125
- w_gate_branch: bfloat16 [2048, 2048], P(None, 'tp'), may hold values from -0.125 to 0.125
- conv_taps: bfloat16 [4, 2048], P(None, 'tp'), may hold values from -3 to 3
- recur_gate_w: bfloat16 [32, 64, 64], P('tp'), may hold values from -0.75 to 0.75
- inject_gate_w: bfloat16 [32, 64, 64], P('tp'), may hold values from -0.75 to 0.75
- decay_logit: float32 [2048], P('tp')
- decay_kick: float32 [8192, 32], P('ep', 'tp'), may hold values from -0.7 to 0
- w_mix_out: bfloat16 [2048, 2048], P('tp'), may hold values from -0.125 to 0.125
- moe_tokens: bfloat16 [4096, 2048], P(('ep', 'tp')), may hold values from -6 to 6
- moe_gain: bfloat16 [2048], replicated, may hold values from 0.099609375 to 1.8984375
- expert_ids: int32 [4096, 2], P(('ep', 'tp')), may hold values from 0 to 7, all different within a row; in each aligned block of 128 rows (0 to 127, 128 to 255, ...) at most 64 rows name the same one
- route_weight: float32 [4096, 2], P(('ep', 'tp')), may hold values from 0.1 to 1
- expert_gate_w: bfloat16 [8, 2048, 1024], P('ep', None, 'tp'), may hold values from -0.125 to 0.125
- expert_up_w: bfloat16 [8, 2048, 1024], P('ep', None, 'tp'), may hold values from -0.125 to 0.125
- expert_down_w: bfloat16 [8, 1024, 2048], P('ep', 'tp'), may hold values from -0.1875 to 0.1875
Outputs:
- mixer_out: bfloat16 [8192, 2048], P(('ep', 'tp'))
- expert_out: bfloat16 [4096, 2048], P(('ep', 'tp'))
The draws below stay inside these ranges and needn't reach their ends.
Inputs may be any that keep to these rules, and one draw needn't show every extreme that they name: `expert_ids`: each row names 2 different experts. In each aligned block of 128 rows (the rows of one device) no expert is named more than 64 times, a bound that some block reaches.
All inputs are finite; a program needn't handle non-finite values.
Results may differ from the reference program's by a relative error of at most 0.015.
Values may be sent and summed in bfloat16 or wider, within the bound.
No kernel may reach another device: no remote copies, remote signals or barrier semaphores. Data moves between devices by JAX's collectives and lax.ppermute only.
A program may use at most 128 MiB of HBM per device.

```python
import math
import jax
import jax.numpy as jnp
import numpy as np
from jax import lax

D = 2048
RECURRENT_HEADS = 32
HEAD_DIM = 64
B_WIDTH = 2048
CONV = 4
FF = 1024
TOP_K = 2
MIX_DEV = 256
MOE_DEV = 128
MIXER_TOKENS = 8192
MOE_TOKENS = 4096
EXPERTS = 8
CAP = 64
N_TP = 4


def draw_decay_logit(key, part):
    fast_key, rate_key = jax.random.split(jax.random.fold_in(key, 11))
    share = 0.5
    fast_mask = jax.random.uniform(fast_key, (B_WIDTH,), jnp.float32) < share
    unit_draw = jax.random.uniform(rate_key, (B_WIDTH,), jnp.float32)
    fast_rate = jnp.exp(jnp.log(1.0 / 400.0) + unit_draw * jnp.log(400.0 / 120.0))
    slow_rate = jnp.exp(jnp.log(0.05) + unit_draw * jnp.log(2.0)) / MIXER_TOKENS
    step_rate = jnp.where(fast_mask, fast_rate, slow_rate)
    return (-jnp.log(jnp.expm1(step_rate))).astype(jnp.float32)


def draw_decay_kick(key, part):
    rate_key, location_random_key, size_random_key = jax.random.split(jax.random.fold_in(key, 23), 3)
    blocks = MIXER_TOKENS // MIX_DEV
    per_block = jnp.exp(jnp.log(0.5) + jnp.log(4.0) * jax.random.uniform(rate_key, (blocks, 1), jnp.float32))
    block_offset = jnp.repeat(-0.5 * per_block / MIXER_TOKENS, MIX_DEV, axis=0) * jnp.ones((1, RECURRENT_HEADS), jnp.float32)
    spike_locations = jax.random.randint(location_random_key, (3, RECURRENT_HEADS), 0, MIXER_TOKENS)
    spike_depth = jnp.log(jax.random.uniform(size_random_key, (3, RECURRENT_HEADS), jnp.float32, 0.55, 0.8))
    token_position = jnp.arange(MIXER_TOKENS, dtype=jnp.int32)[:, None]
    spike_events = jnp.zeros((MIXER_TOKENS, RECURRENT_HEADS), jnp.float32)
    for index_value in range(3):
        spike_events = spike_events + jnp.where(token_position == spike_locations[index_value][None, :], spike_depth[index_value][None, :], 0.0)
    return (block_offset + spike_events).astype(jnp.float32)


def shard_levels(rng, extent, cuts, smallest, largest):
    level, own = 1.0, jax.random.fold_in(rng, 6)
    for position, shards_of in cuts:
        steps = jnp.exp(jax.random.uniform(jax.random.fold_in(own, position), (shards_of,), jnp.float32, smallest / len(cuts), largest / len(cuts)))
        level = level * jnp.repeat(steps, extent[position] // shards_of).reshape([-1 if axis == position else 1 for axis in range(len(extent))])
    return level


def assign_block(own_key, own, number, rows, count, top, limit, slope):
    order = jax.random.permutation(own_key, count)
    crowded, ordinary = load_shares(count, rows * top, limit, slope, True), load_shares(count, rows * top, limit, slope, False)
    places = jnp.arange(count)

    def named(tallies, offset_by):
        used = int((tallies > 0).sum())
        fixed = max(1, used // 4)
        shifted = fixed + (places - fixed + offset_by * (used - fixed)) % max(1, count - fixed)
        return jnp.zeros((count,), jnp.int32).at[order[jnp.where(places < fixed, places, shifted)]].set(jnp.asarray(tallies, jnp.int32))

    tallies = jnp.where(number % 4 == 0, named(crowded, number // 4), named(ordinary, number - number // 4 - 1))
    mixed = jax.random.permutation(jax.random.fold_in(own, 3), count)
    donor, receiver = mixed[0:count // 2 * 2:2], mixed[1:count // 2 * 2:2]
    margin = jnp.minimum(tallies[donor] - 1, limit - tallies[receiver]) // 2
    margin = jnp.where((donor == order[0]) | (receiver == order[0]) | (tallies[receiver] == 0), 0, jnp.maximum(margin, 0))
    shifted = jax.random.randint(jax.random.fold_in(own, 4), (count // 2,), 0, 1 << 20) % (margin + 1)
    tallies = tallies.at[donor].add(-shifted).at[receiver].add(shifted)
    labels = jnp.searchsorted(jnp.cumsum(tallies), jnp.arange(rows * top), side="right").astype(jnp.int32)
    grid = labels.reshape(top, rows).T
    grid = grid[jax.random.permutation(jax.random.fold_in(own, 1), rows)]
    offset_by = jax.random.randint(jax.random.fold_in(own, 2), (rows, 1), 0, top)
    return jnp.take_along_axis(grid, (jnp.arange(top)[None, :] + offset_by) % top, axis=1)


def load_shares(number_of, total, bound, slope, full):
    weights = [(1 << 20) // math.isqrt(rank ** slope) + 1 for rank in range(1, number_of + 1)]
    largest = bound if full else min(bound, max(-(-total // number_of), total * weights[0] // sum(weights)))
    least = 1 if total - largest >= number_of - 1 else 0
    counts, spare = [largest] + [least] * (number_of - 1), total - largest - least * (number_of - 1)
    while spare > 0:
        candidates = [i for i in range(1, number_of) if counts[i] < largest] or [i for i in range(1, number_of) if counts[i] < bound]
        pool, left = sum([weights[i] for i in candidates]), spare
        for i in candidates:
            addition = min(bound - counts[i], max(1, left * weights[i] // pool), spare)
            counts[i] = counts[i] + addition
            spare = spare - addition
    return np.array(counts)


def centred(own_key, extent, width, bound, pieces=(), kind=jnp.bfloat16):
    drawn = jax.random.normal(own_key, extent, jnp.float32) * width
    if len(pieces) > 0:
        drawn = shard_levels(own_key, extent, pieces, -0.22, 0.18) * drawn
    return jnp.clip(drawn, min=-bound, max=bound).astype(kind)


def setup_inputs(seed: int = 0) -> dict:
    streams_of = jax.random.split(jax.random.key(seed), 18)
    mix_tokens = centred(streams_of[0], (MIXER_TOKENS, D), 1.0, 6.0, ((0, 32),))
    mix_gain = jnp.clip(1.0 + 0.18 * jax.random.normal(streams_of[1], (D,), jnp.float32), 0.099609375, 1.8984375).astype(jnp.bfloat16)
    w_branch = centred(streams_of[2], (D, B_WIDTH), D ** -0.5, 0.125, ((1, 4),))
    w_gate_branch = centred(streams_of[3], (D, B_WIDTH), D ** -0.5, 0.125, ((1, 4),))
    conv_taps = centred(streams_of[4], (CONV, B_WIDTH), CONV ** -0.5, 3.0, ((1, 4),))
    recur_gate_w = centred(streams_of[5], (RECURRENT_HEADS, HEAD_DIM, HEAD_DIM), HEAD_DIM ** -0.5, 0.75, ((0, 4),))
    inject_gate_w = centred(streams_of[6], (RECURRENT_HEADS, HEAD_DIM, HEAD_DIM), HEAD_DIM ** -0.5, 0.75, ((0, 4),))
    decay_logit = draw_decay_logit(jax.random.fold_in(streams_of[17], 71), 0)
    decay_kick = draw_decay_kick(jax.random.fold_in(streams_of[17], 71), 0)
    w_mix_out = centred(streams_of[9], (B_WIDTH, D), B_WIDTH ** -0.5, 0.125, ((0, 4),))
    moe_tokens = centred(streams_of[10], (MOE_TOKENS, D), 1.0, 6.0, ((0, 32),))
    moe_gain = jnp.clip(1.0 + 0.18 * jax.random.normal(streams_of[11], (D,), jnp.float32), 0.099609375, 1.8984375).astype(jnp.bfloat16)
    expert_ids_keys = jax.random.split(jax.random.fold_in(streams_of[12], 1), MOE_TOKENS // MOE_DEV)
    expert_ids_turns = jax.random.permutation(jax.random.fold_in(streams_of[12], 3), MOE_TOKENS // MOE_DEV)
    expert_ids = jax.vmap(lambda own, number: assign_block(jax.random.fold_in(streams_of[12], 2), own, number, MOE_DEV, EXPERTS, TOP_K, CAP, 1))(expert_ids_keys, expert_ids_turns).reshape((MOE_TOKENS, TOP_K))
    route_weight = jnp.clip(jnp.exp(math.log(1.0) - 2.3025851 * jax.random.uniform(streams_of[13], (MOE_TOKENS, TOP_K), jnp.float32) ** shard_levels(streams_of[13], (MOE_TOKENS, TOP_K), ((0, 32),), -0.2, 0.2)), 0.1, 1.0)
    expert_gate_w = centred(streams_of[14], (EXPERTS, D, FF), D ** -0.5, 0.125, ((0, 8), (2, 4)))
    expert_up_w = centred(streams_of[15], (EXPERTS, D, FF), D ** -0.5, 0.125, ((0, 8), (2, 4)))
    expert_down_w = centred(streams_of[16], (EXPERTS, FF, D), FF ** -0.5, 0.1875, ((0, 8), (1, 4)))
    return dict(mix_tokens=mix_tokens, mix_gain=mix_gain, w_branch=w_branch, w_gate_branch=w_gate_branch, conv_taps=conv_taps, recur_gate_w=recur_gate_w, inject_gate_w=inject_gate_w, decay_logit=decay_logit, decay_kick=decay_kick, w_mix_out=w_mix_out, moe_tokens=moe_tokens, moe_gain=moe_gain, expert_ids=expert_ids, route_weight=route_weight, expert_gate_w=expert_gate_w, expert_up_w=expert_up_w, expert_down_w=expert_down_w)


epsilon = 1e-06
gate_const = 8.0

def norm_rows(values, gain_vec):
    value_f32 = values.astype(jnp.float32)
    inv_scale = lax.rsqrt(lax.optimization_barrier(jnp.mean(value_f32 * value_f32, axis=-1, keepdims=True)) + epsilon)
    return (value_f32 * inv_scale * gain_vec.astype(jnp.float32)).astype(jnp.bfloat16)

def chain_link(earlier, later):
    return (later[0] * earlier[0], later[0] * earlier[1] + later[1])

def reference(mix_tokens, mix_gain, w_branch, w_gate_branch, conv_taps, recur_gate_w, inject_gate_w, decay_logit, decay_kick, w_mix_out, moe_tokens, moe_gain, expert_ids, route_weight, expert_gate_w, expert_up_w, expert_down_w):
    mixer_in = norm_rows(mix_tokens, mix_gain)
    branch_x = jnp.dot(mixer_in, w_branch, preferred_element_type=jnp.float32).astype(jnp.bfloat16)
    branch_gate = jnp.dot(mixer_in, w_gate_branch, preferred_element_type=jnp.float32).astype(jnp.bfloat16)
    branch_f32 = branch_x.astype(jnp.float32)
    tap_values = conv_taps.astype(jnp.float32)
    padded = jnp.pad(branch_f32, ((CONV - 1, 0), (0, 0)))
    conv_out = tap_values[CONV - 1] * branch_f32
    for index_value in range(CONV - 1):
        conv_out = conv_out + tap_values[index_value] * padded[index_value:index_value + MIXER_TOKENS]
    conv_low = lax.optimization_barrier(conv_out.astype(jnp.bfloat16))
    low_heads = conv_low.astype(jnp.float32).reshape(MIXER_TOKENS, RECURRENT_HEADS, HEAD_DIM)
    recur = jax.nn.sigmoid(jnp.einsum('thi,hij->thj', low_heads, recur_gate_w.astype(jnp.float32)).reshape(MIXER_TOKENS, B_WIDTH))
    inject = jax.nn.sigmoid(jnp.einsum('thi,hij->thj', low_heads, inject_gate_w.astype(jnp.float32)).reshape(MIXER_TOKENS, B_WIDTH))
    slowness = jax.nn.softplus(-decay_logit)
    kick_wide = jnp.repeat(decay_kick, HEAD_DIM, axis=1)
    log_decay = -gate_const * recur * slowness[None, :] + kick_wide
    drive = jnp.sqrt(-jnp.expm1(2.0 * log_decay)) * inject * conv_out
    _, state = lax.associative_scan(chain_link, (jnp.exp(log_decay), drive), axis=0)
    mixed = (state * jax.nn.gelu(branch_gate.astype(jnp.float32))).astype(jnp.bfloat16)
    col_count = B_WIDTH // N_TP
    summed = jnp.zeros((MIXER_TOKENS, D), jnp.float32)
    for group in range(N_TP):
        piece = jnp.dot(mixed[:, group * col_count:(group + 1) * col_count], w_mix_out[group * col_count:(group + 1) * col_count], preferred_element_type=jnp.float32)
        summed = summed + lax.optimization_barrier(piece.astype(jnp.bfloat16)).astype(jnp.float32)
    mixer_out = summed.astype(jnp.bfloat16)
    moe_in = norm_rows(moe_tokens, moe_gain)
    blocks = MOE_TOKENS // MOE_DEV
    route_ids = expert_ids.reshape(blocks, MOE_DEV * TOP_K)
    onehot = (route_ids[:, :, None] == jnp.arange(EXPERTS, dtype=jnp.int32)[None, None, :]).astype(jnp.int32)
    earlier_count = jnp.cumsum(onehot, axis=1) - onehot
    slot_index = lax.optimization_barrier(jnp.sum(earlier_count * onehot, axis=2))
    per_expert = blocks * CAP
    slot_target = (route_ids * per_expert + jnp.arange(blocks, dtype=jnp.int32)[:, None] * CAP + slot_index).reshape(-1).astype(jnp.int32)
    source = jnp.repeat(moe_in, TOP_K, axis=0)
    buffer = jnp.zeros((EXPERTS * per_expert, D), jnp.bfloat16).at[slot_target].set(source)
    quarter = FF // N_TP

    def run_expert(operands):
        expert_rows, gate_mat, up_mat, down_mat = operands
        hidden = (jax.nn.silu(jnp.dot(expert_rows, gate_mat, preferred_element_type=jnp.float32)) * jnp.dot(expert_rows, up_mat, preferred_element_type=jnp.float32)).astype(jnp.bfloat16)
        summed_rows = jnp.zeros((expert_rows.shape[0], D), jnp.float32)
        for group in range(N_TP):
            piece = jnp.dot(hidden[:, group * quarter:(group + 1) * quarter], down_mat[group * quarter:(group + 1) * quarter], preferred_element_type=jnp.float32)
            summed_rows = summed_rows + lax.optimization_barrier(piece.astype(jnp.bfloat16)).astype(jnp.float32)
        return summed_rows.astype(jnp.bfloat16)
    results = lax.map(run_expert, (buffer.reshape(EXPERTS, per_expert, D), expert_gate_w, expert_up_w, expert_down_w))
    results = results.reshape(EXPERTS * per_expert, D)
    picked = results[slot_target].astype(jnp.float32).reshape(MOE_TOKENS, TOP_K, D)
    expert_out = lax.optimization_barrier(jnp.sum(picked * route_weight[:, :, None], axis=1)).astype(jnp.bfloat16)
    return (mixer_out, expert_out)
```

```python
import functools

import jax
import jax.numpy as jnp
from jax import lax
from jax.experimental import pallas as pl
from jax.experimental.pallas import tpu as pltpu
from jax.sharding import PartitionSpec as P


epsilon = 1e-06
gate_const = 8.0
SUB = 8
F32 = jnp.float32
BF16 = jnp.bfloat16


def dotf(a, b):
    return jnp.dot(a, b, preferred_element_type=F32)


def swap(block, axis, bit):
    size = lax.axis_size(axis)
    return lax.ppermute(block, axis, [(i, i ^ bit) for i in range(size)])


def from_behind(block, axis, distance):
    size = lax.axis_size(axis)
    return lax.ppermute(block, axis, [(i, i + distance) for i in range(size - distance)])


def tp_bits():
    size, bits = lax.axis_size("tp"), []
    while size > 1:
        size //= 2
        bits.append(size)
    return bits


def spread(block):
    held = {0: block}
    for bit in tp_bits():
        held.update({k ^ bit: swap(v, "tp", bit) for k, v in list(held.items())})
    return [held[k] for k in range(len(held))]


def norm_rows(values, gain_vec):
    value_f32 = values.astype(F32)
    inv_scale = lax.rsqrt(jnp.mean(value_f32 * value_f32, axis=-1, keepdims=True) + epsilon)
    return (value_f32 * inv_scale * gain_vec.astype(F32)).astype(BF16)


def cost(flops, moved, transcendentals=0):
    return pl.CostEstimate(flops=flops, bytes_accessed=moved, transcendentals=transcendentals)


def call(kernel, outs, flops, *args, scratch=(), smem=()):
    moved = sum(a.size * a.dtype.itemsize for a in args) + sum(
        o.size * o.dtype.itemsize for o in jax.tree.leaves(outs)
    )
    return pl.pallas_call(
        kernel,
        out_shape=outs,
        in_specs=[
            pl.BlockSpec(memory_space=pltpu.SMEM if i in smem else pltpu.VMEM)
            for i in range(len(args))
        ],
        out_specs=jax.tree.map(lambda o: pl.BlockSpec(memory_space=pltpu.VMEM), outs),
        scratch_shapes=list(scratch),
        cost_estimate=cost(flops, moved),
    )(*args)


def norm_kernel(x_ref, gain_ref, out_ref, tail_ref):
    rows = x_ref.shape[0]
    steps = rows // SUB
    values = x_ref[...].astype(F32)
    inv = lax.rsqrt(jnp.mean(values * values, axis=-1, keepdims=True) + epsilon)
    normed = (values * inv * gain_ref[...].astype(F32)).astype(BF16)
    r = lax.broadcasted_iota(jnp.int32, (rows, rows), 0)
    t = lax.broadcasted_iota(jnp.int32, (rows, rows), 1)
    order = (t == (r % SUB) * steps + r // SUB).astype(F32).astype(BF16)
    out_ref[...] = dotf(order, normed).astype(BF16)
    lead = tail_ref.shape[0]
    r = lax.broadcasted_iota(jnp.int32, (lead, rows), 0)
    t = lax.broadcasted_iota(jnp.int32, (lead, rows), 1)
    pick = (t == r + rows - lead).astype(F32).astype(BF16)
    tail_ref[...] = dotf(pick, normed).astype(BF16)


def block_kernel(
    taps_count,
    x_ref,
    tail_ref,
    wb_ref,
    wg_ref,
    taps_ref,
    gates_ref,
    slow_ref,
    kick_ref,
    loc_ref,
    acc_ref,
    gelu_ref,
    pref_ref,
    tot_ref,
    xf_ref,
    bg_ref,
    conv_ref,
    pre_ref,
):
    rows, cols = loc_ref.shape
    steps = rows // SUB
    lead = taps_count - 1
    x = x_ref[...]
    bx = dotf(x, wb_ref[...]).astype(BF16).astype(F32)
    bt = dotf(tail_ref[...], wb_ref[...]).astype(BF16).astype(F32)
    bt = bt[bt.shape[0] - lead :]
    bg_ref[...] = dotf(x, wg_ref[...]).astype(BF16).astype(F32)
    sub = lax.broadcasted_iota(jnp.int32, (SUB, cols), 0)
    xf_ref[lead * SUB :, :] = bx
    for m in range(lead):
        at = (steps - lead + m) * SUB
        shifted = pltpu.roll(bx[at : at + SUB], 1, 0)
        xf_ref[m * SUB : (m + 1) * SUB, :] = jnp.where(sub == 0, bt[m : m + 1], shifted)
    taps = taps_ref[...].astype(F32)
    conv = taps[lead : lead + 1] * bx
    for k in range(lead):
        conv = conv + taps[k : k + 1] * xf_ref[k * SUB : k * SUB + rows, :]
    conv_ref[...] = conv
    low = conv.astype(BF16)
    width = gates_ref.shape[1]
    for g in range(cols // width):
        pre = dotf(low[:, g * width : (g + 1) * width], gates_ref[g])
        pre_ref[:, g * width : (g + 1) * width] = pre[:, :width]
        pre_ref[:, cols + g * width : cols + (g + 1) * width] = pre[:, width:]
    slow = slow_ref[...] * (-gate_const)

    def step(j, carry):
        state, decay = carry
        at = pl.ds(pl.multiple_of(j * SUB, SUB), SUB)
        recur = jax.nn.sigmoid(pre_ref[at, :cols])
        inject = jax.nn.sigmoid(pre_ref[at, cols:])
        log_decay = recur * slow + kick_ref[at, :]
        a = jnp.exp(log_decay)
        u = 2.0 * log_decay
        series = 1.0 / 40320.0
        for c in (5040.0, 720.0, 120.0, 24.0, 6.0, 2.0, 1.0):
            series = series * u + 1.0 / c
        gone = jnp.where(u > -0.5, -u * series, 1.0 - a * a)
        drive = jnp.sqrt(gone) * inject * conv_ref[at, :]
        state = a * state + drive
        decay = a * decay
        loc_ref[at, :] = state
        acc_ref[at, :] = decay
        gelu_ref[at, :] = jax.nn.gelu(bg_ref[at, :])
        return state, decay

    unroll = 4 if steps % 4 == 0 else 1

    def several(i, carry):
        for n in range(unroll):
            carry = step(i * unroll + n, carry)
        return carry

    state, decay = lax.fori_loop(
        0,
        steps // unroll,
        several,
        (jnp.zeros((SUB, cols), F32), jnp.ones((SUB, cols), F32)),
    )
    for d in (1, 2, 4):
        behind_state = pltpu.roll(state, d, 0)
        behind_decay = pltpu.roll(decay, d, 0)
        state = jnp.where(sub >= d, decay * behind_state + state, state)
        decay = jnp.where(sub >= d, decay * behind_decay, decay)
    pref_ref[:SUB, :] = jnp.where(sub == 0, 0.0, pltpu.roll(state, 1, 0))
    pref_ref[SUB:, :] = jnp.where(sub == 0, 1.0, pltpu.roll(decay, 1, 0))
    tot_ref[0:1, :] = decay[SUB - 1 :]
    tot_ref[1:2, :] = state[SUB - 1 :]


def chain(decay, state, part):
    return part[0:1] * decay, part[0:1] * state + part[1:2]


def choose(parts, index):
    picked = parts[0]
    for k in range(1, len(parts)):
        picked = jnp.where(index == k, parts[k], picked)
    return picked


def total_kernel(count, place_ref, *refs):
    tots, out_ref = [r[...] for r in refs[:count]], refs[count]
    me = place_ref[0]
    decay = jnp.ones((1, out_ref.shape[2]), F32)
    state = jnp.zeros((1, out_ref.shape[2]), F32)
    for b in range(count):
        decay, state = chain(decay, state, choose(tots, me ^ b))
    for i in range(out_ref.shape[0]):
        out_ref[i, 0:1, :] = decay
        out_ref[i, 1:2, :] = state


def out_kernel(count, ks, kinds, place_ref, ends_ref, *refs):
    tots = [r[...] for r in refs[:count]]
    rest = refs[count:]
    n = len(ks)
    locs, accs, gelus, prefs = rest[:n], rest[n : 2 * n], rest[2 * n : 3 * n], rest[3 * n : 4 * n]
    w_ref, outs = rest[4 * n], rest[4 * n + 1 :]
    me, here = place_ref[0], place_ref[1]
    cols = w_ref.shape[0]

    def one(i, state):
        part = ends_ref[i]
        return part[0:1] * state + part[1:2]

    entry = lax.fori_loop(0, here, one, jnp.zeros((1, cols), F32))
    entries = []
    decay = jnp.ones((1, cols), F32)
    for b in range(count):
        entries.append(entry)
        decay, entry = chain(decay, entry, choose(tots, me ^ b))
    for i, k in enumerate(ks):
        carried = choose(entries, me ^ k)
        rows = locs[i].shape[0]
        pref = prefs[i][...]
        lift = pref[:SUB] + pref[SUB:] * carried
        lift = jnp.broadcast_to(lift[None], (rows // SUB, SUB, cols)).reshape(rows, cols)
        mixed = ((locs[i][...] + accs[i][...] * lift) * gelus[i][...]).astype(BF16)
        outs[i][...] = dotf(mixed, w_ref[...]).astype(outs[i].dtype)


def add_kernel(a_ref, b_ref, out_ref):
    out_ref[...] = (a_ref[...].astype(F32) + b_ref[...].astype(F32)).astype(BF16)


def last_kernel(a_ref, b_ref, c_ref, out_ref):
    rows = out_ref.shape[0]
    steps = rows // SUB
    total = a_ref[...].astype(F32) + b_ref[...].astype(F32) + c_ref[...].astype(F32)
    t = lax.broadcasted_iota(jnp.int32, (rows, rows), 0)
    r = lax.broadcasted_iota(jnp.int32, (rows, rows), 1)
    order = (t == (r % SUB) * steps + r // SUB).astype(F32).astype(BF16)
    out_ref[...] = dotf(order, total.astype(BF16)).astype(BF16)


def block_diagonal(head_maps):
    head_count, head_dim, _ = head_maps.shape
    head_eye = jnp.eye(head_count, dtype=head_maps.dtype)
    wide = head_maps[:, :, None, :] * head_eye[:, None, :, None]
    return wide.reshape(head_count * head_dim, head_count * head_dim)


def hidden_kernel(n, x_ref, *refs):
    x = x_ref[...]
    for i in range(n):
        gate = dotf(x, refs[i][...])
        up = dotf(x, refs[n + i][...])
        refs[2 * n + i][...] = (jax.nn.silu(gate) * up).astype(BF16)


def down_kernel(n, *refs):
    out_ref = refs[2 * n]
    total = dotf(refs[0][...], refs[n][...])
    for i in range(1, n):
        total = total + dotf(refs[i][...], refs[n + i][...])
    out_ref[...] = total.astype(BF16)


def body(
    mix_tokens,
    mix_gain,
    w_branch,
    w_gate_branch,
    conv_taps,
    recur_gate_w,
    inject_gate_w,
    decay_logit,
    decay_kick,
    w_mix_out,
    moe_tokens,
    moe_gain,
    expert_ids,
    route_weight,
    expert_gate_w,
    expert_up_w,
    expert_down_w,
):
    shape = jax.ShapeDtypeStruct
    me = lax.axis_index("tp")
    here = lax.axis_index("ep")
    place = jnp.stack([me, here]).astype(jnp.int32)
    count = lax.axis_size("tp")
    ep_size = lax.axis_size("ep")
    rows, width = mix_tokens.shape
    cols = w_branch.shape[1]
    taps_count = conv_taps.shape[0]
    steps = rows // SUB

    mixer_in, tail = call(
        norm_kernel,
        (shape((rows, width), BF16), shape((SUB, width), BF16)),
        2 * rows * rows * width,
        mix_tokens,
        mix_gain[None, :],
    )
    tails = spread(tail)
    blocks = spread(mixer_in)

    moe_in = norm_rows(moe_tokens, moe_gain)
    local_rows, top_count = expert_ids.shape
    room = 2 * local_rows * top_count // ep_size
    flat_ids = expert_ids.reshape(-1)
    onehot = (flat_ids[:, None] == jnp.arange(ep_size, dtype=jnp.int32)[None, :]).astype(jnp.int32)
    earlier_count = jnp.cumsum(onehot, axis=0) - onehot
    slot_index = jnp.sum(earlier_count * onehot, axis=1)
    slot_target = (flat_ids * room + slot_index).reshape(local_rows, top_count)
    slots_total = ep_size * room
    slot_range = jnp.arange(slots_total, dtype=jnp.int32)
    picks = [(slot_target[:, k][:, None] == slot_range[None, :]) for k in range(top_count)]
    table = functools.reduce(jnp.logical_or, picks).astype(BF16)
    outgoing = lax.dot_general(
        table, moe_in, (((0,), (0,)), ((), ())), preferred_element_type=F32
    ).astype(BF16)
    arrived = lax.all_to_all(outgoing, "ep", split_axis=0, concat_axis=0, tiled=True)

    gate_parts = spread(expert_gate_w[0])
    up_parts = spread(expert_up_w[0])
    down = expert_down_w[0]
    halves = 2
    span = down.shape[1] // halves
    down_parts = [spread(down[:, i * span : (i + 1) * span]) for i in range(halves)]

    head_count, head_dim, _ = recur_gate_w.shape
    group = 256 if cols % 256 == 0 and 256 % head_dim == 0 else cols
    per = group // head_dim
    gates = jnp.stack(
        [
            jnp.concatenate(
                [
                    block_diagonal(recur_gate_w[g * per : (g + 1) * per]),
                    block_diagonal(inject_gate_w[g * per : (g + 1) * per]),
                ],
                axis=1,
            )
            for g in range(cols // group)
        ]
    )
    slowness = jax.nn.softplus(-decay_logit)[None, :]
    widen = (
        jnp.arange(cols, dtype=jnp.int32)[None, :] // head_dim
        == jnp.arange(head_count, dtype=jnp.int32)[:, None]
    ).astype(F32)
    kick = decay_kick.reshape(count, SUB, steps, head_count).swapaxes(1, 2)
    kick = jnp.dot(
        kick.reshape(count * rows, head_count), widen, precision=lax.Precision.HIGHEST
    ).reshape(count, rows, cols)
    tail_of = jnp.stack(tails)
    before = from_behind(tail_of[me ^ (count - 1)], "ep", 1)

    parts = []
    for k in range(count):
        number = me ^ k
        lead_rows = jnp.where(number == 0, before, tail_of[me ^ jnp.maximum(number - 1, 0)])
        parts.append(
            call(
                functools.partial(block_kernel, taps_count),
                (
                    shape((rows, cols), F32),
                    shape((rows, cols), F32),
                    shape((rows, cols), F32),
                    shape((2 * SUB, cols), F32),
                    shape((2, cols), F32),
                ),
                2 * rows * cols * (2 * width + 2 * group),
                blocks[k],
                lead_rows,
                w_branch,
                w_gate_branch,
                conv_taps,
                gates,
                slowness,
                kick[number],
                scratch=(
                    pltpu.VMEM((rows + (taps_count - 1) * SUB, cols), F32),
                    pltpu.VMEM((rows, cols), F32),
                    pltpu.VMEM((rows, cols), F32),
                    pltpu.VMEM((rows, 2 * cols), F32),
                ),
            )
        )
    tots = [p[4] for p in parts]
    ends = call(
        functools.partial(total_kernel, count),
        shape((ep_size, 2, cols), F32),
        1000,
        place,
        *tots,
        smem=(0,),
    )
    ends = lax.all_to_all(ends, "ep", split_axis=0, concat_axis=0, tiled=True)

    def project(ks, kinds):
        return call(
            functools.partial(out_kernel, count, ks, kinds),
            tuple(shape((rows, width), kind) for kind in kinds),
            2 * len(ks) * rows * cols * width,
            place,
            ends,
            *tots,
            *[parts[k][0] for k in ks],
            *[parts[k][1] for k in ks],
            *[parts[k][2] for k in ks],
            *[parts[k][3] for k in ks],
            w_mix_out,
            smem=(0,),
        )

    far_other, far_same = project((3, 2), (BF16, BF16))
    near_other, near_same = project((1, 0), (BF16, BF16))
    far_sum = call(
        add_kernel,
        shape((rows, width), BF16),
        rows * width,
        far_same,
        swap(far_other, "tp", 1),
    )
    mixer_out = call(
        last_kernel,
        shape((rows, width), BF16),
        2 * rows * rows * width,
        near_same,
        swap(near_other, "tp", 1),
        swap(far_sum, "tp", 2),
    )

    hidden = []
    for ks in ((0, 1), (2, 3)):
        hidden += call(
            functools.partial(hidden_kernel, len(ks)),
            tuple(shape((slots_total, gate_parts[0].shape[1]), BF16) for _ in ks),
            4 * len(ks) * slots_total * width * gate_parts[0].shape[1],
            arrived,
            *[gate_parts[k] for k in ks],
            *[up_parts[k] for k in ks],
        )
    returned = []
    for i in range(halves):
        done = call(
            functools.partial(down_kernel, count),
            shape((slots_total, span), BF16),
            2 * slots_total * span * count * down.shape[0],
            *hidden,
            *down_parts[i],
        )
        returned.append(lax.all_to_all(done, "ep", split_axis=0, concat_axis=0, tiled=True))
    weighted = jnp.zeros((local_rows, slots_total), F32)
    for k in range(top_count):
        weighted = weighted + picks[k].astype(F32) * route_weight[:, k][:, None]
    expert_out = jnp.concatenate(
        [
            jnp.dot(weighted, r.astype(F32), precision=lax.Precision.HIGHEST).astype(BF16)
            for r in returned
        ],
        axis=1,
    )
    return (mixer_out, expert_out)


def solution(mesh):
    placed = (
        P(("ep", "tp"), None),
        P(),
        P(None, "tp"),
        P(None, "tp"),
        P(None, "tp"),
        P("tp", None, None),
        P("tp", None, None),
        P("tp"),
        P("ep", "tp"),
        P("tp", None),
        P(("ep", "tp"), None),
        P(),
        P(("ep", "tp"), None),
        P(("ep", "tp"), None),
        P("ep", None, "tp"),
        P("ep", None, "tp"),
        P("ep", "tp", None),
    )
    return jax.shard_map(
        body,
        mesh=mesh,
        in_specs=placed,
        out_specs=(P(("ep", "tp"), None), P(("ep", "tp"), None)),
        check_vma=False,
    )
```

```python
import functools
import math

import jax
import jax.numpy as jnp
from jax import lax
from jax.experimental import pallas as pl
from jax.experimental.pallas import tpu as pltpu
from jax.sharding import PartitionSpec as P


epsilon = 1e-06
gate_const = 8.0
SUB = 8
SPARE = 6
F32 = jnp.float32
BF16 = jnp.bfloat16


def dotf(a, b):
    return jnp.dot(a, b, preferred_element_type=F32)


def swap(block, axis, bit):
    size = lax.axis_size(axis)
    return lax.ppermute(block, axis, [(i, i ^ bit) for i in range(size)])


def from_behind(block, axis, distance):
    size = lax.axis_size(axis)
    return lax.ppermute(block, axis, [(i, i + distance) for i in range(size - distance)])


def exchange(block, axis):
    return lax.all_to_all(block, axis, split_axis=0, concat_axis=0, tiled=True)


def tp_bits():
    size, bits = lax.axis_size("tp"), []
    while size > 1:
        size //= 2
        bits.append(size)
    return bits


def spread(block):
    held = {0: block}
    for bit in tp_bits():
        held.update({k ^ bit: swap(v, "tp", bit) for k, v in list(held.items())})
    return [held[k] for k in range(len(held))]


def cost(flops, moved, transcendentals=0):
    return pl.CostEstimate(flops=flops, bytes_accessed=moved, transcendentals=transcendentals)


def call(kernel, outs, flops, *args, scratch=(), smem=(), alone=False):
    sizes = [a.size * a.dtype.itemsize for a in args]
    sizes += [o.size * o.dtype.itemsize for o in jax.tree.leaves(outs)]
    moved = sum(sizes)
    held = moved + sum(math.prod(v.shape) * jnp.dtype(v.dtype).itemsize for v in scratch)
    return pl.pallas_call(
        kernel,
        out_shape=outs,
        in_specs=[
            pl.BlockSpec(memory_space=pltpu.SMEM if i in smem else pltpu.VMEM)
            for i in range(len(args))
        ],
        out_specs=jax.tree.map(lambda o: pl.BlockSpec(memory_space=pltpu.VMEM), outs),
        scratch_shapes=list(scratch),
        cost_estimate=cost(flops, moved),
        compiler_params=pltpu.CompilerParams(
            vmem_limit_bytes=None if alone else held + (SPARE << 20)
        ),
    )(*args)


def normed_rows(x_ref, gain_ref):
    values = x_ref[...].astype(F32)
    inv = lax.rsqrt(jnp.mean(values * values, axis=-1, keepdims=True) + epsilon)
    return (values * inv * gain_ref[...][None, :].astype(F32)).astype(BF16)


def norm_kernel(x_ref, before_ref, gain_ref, out_ref, tail_ref):
    rows = x_ref.shape[0]
    steps = rows // SUB
    normed = normed_rows(x_ref, gain_ref)
    r = lax.broadcasted_iota(jnp.int32, (rows, rows), 0)
    t = lax.broadcasted_iota(jnp.int32, (rows, rows), 1)
    order = (t == (r % SUB) * steps + r // SUB).astype(F32).astype(BF16)
    out_ref[...] = dotf(order, normed).astype(BF16)
    lead = before_ref.shape[0]
    tail_ref[:lead] = normed[rows - lead :]
    tail_ref[lead:] = normed_rows(before_ref, gain_ref)


def split3(values):
    high = values.astype(BF16)
    rest = values - high.astype(F32)
    middle = rest.astype(BF16)
    return high, middle, (rest - middle.astype(F32)).astype(BF16)


def gates_kernel(recur_ref, inject_ref, out_ref):
    groups, width, _ = out_ref.shape
    head = recur_ref.shape[1]
    j = lax.broadcasted_iota(jnp.int32, (head, width), 0)
    c = lax.broadcasted_iota(jnp.int32, (head, width), 1)
    repeat = (c % head == j).astype(F32).astype(BF16)
    r = lax.broadcasted_iota(jnp.int32, (width, width), 0)
    c = lax.broadcasted_iota(jnp.int32, (width, width), 1)
    same = r // head == c // head
    for g in range(groups):
        for i, ref in enumerate((recur_ref, inject_ref)):
            wide = dotf(ref[g * width : (g + 1) * width, :], repeat)
            out_ref[g, :, i * width : (i + 1) * width] = jnp.where(same, wide, 0.0).astype(BF16)


def block_kernel(taps_count, ks, place_ref, *refs):
    count = refs[0].shape[0]
    n = len(ks)
    kick_ref, wb_ref, wg_ref, taps_ref, gates_ref, slow_ref = refs[:6]
    tails = refs[6 : 6 + count]
    xs = refs[6 + count : 6 + count + n]
    body_ref, edge_ref = refs[6 + count + n : 8 + count + n]
    scratch = refs[8 + count + n :]
    me = place_ref[0]
    for i, k in enumerate(ks):
        number = me ^ k
        half = tails[0].shape[0] // 2
        lead_rows = jnp.zeros((half, tails[0].shape[1]), BF16)
        for other in range(count):
            own, before = tails[other][:half], tails[other][half:]
            lead_rows = jnp.where((me ^ other) + 1 == number, own, lead_rows)
            first = (number == 0) & (me ^ other == count - 1)
            lead_rows = jnp.where(first, before, lead_rows)
        one_block(
            taps_count,
            xs[i],
            lead_rows,
            kick_ref[number],
            wb_ref,
            wg_ref,
            taps_ref,
            gates_ref,
            slow_ref,
            body_ref.at[i],
            edge_ref.at[i],
            *scratch,
        )


def one_block(
    taps_count,
    x_ref,
    lead_rows,
    kicks,
    wb_ref,
    wg_ref,
    taps_ref,
    gates_ref,
    slow_ref,
    body_ref,
    edge_ref,
    xf_ref,
    bg_ref,
    pre_ref,
    wide_ref,
):
    _, rows, cols = body_ref.shape
    steps = rows // SUB
    lead = taps_count - 1
    x = x_ref[...]
    bt = dotf(lead_rows, wb_ref[...]).astype(BF16).astype(F32)
    bt = bt[bt.shape[0] - lead :]
    xf_ref[lead * SUB :, :] = dotf(x, wb_ref[...]).astype(BF16).astype(F32)
    sub = lax.broadcasted_iota(jnp.int32, (SUB, cols), 0)
    for m in range(lead):
        at = rows + m * SUB
        shifted = pltpu.roll(xf_ref[at : at + SUB, :], 1, 0)
        xf_ref[m * SUB : (m + 1) * SUB, :] = jnp.where(sub == 0, bt[m : m + 1], shifted)
    taps = taps_ref[...].astype(F32)
    conv = taps[0:1] * xf_ref[:rows, :]
    for k in range(1, taps_count):
        conv = conv + taps[k : k + 1] * xf_ref[k * SUB : k * SUB + rows, :]
    xf_ref[:rows, :] = conv
    low = conv.astype(BF16)
    width = gates_ref.shape[1]
    for g in range(cols // width):
        pre = dotf(low[:, g * width : (g + 1) * width], gates_ref[g])
        pre_ref[:, g * width : (g + 1) * width] = pre[:, :width]
        pre_ref[:, cols + g * width : cols + (g + 1) * width] = pre[:, width:]
    heads = kicks.shape[1]
    h = lax.broadcasted_iota(jnp.int32, (heads, cols), 0)
    c = lax.broadcasted_iota(jnp.int32, (heads, cols), 1)
    widen = (c // (cols // heads) == h).astype(F32).astype(BF16)
    high, middle, small = split3(kicks)
    wide_ref[...] = dotf(high, widen) + (dotf(middle, widen) + dotf(small, widen))
    bg_ref[...] = dotf(x, wg_ref[...]).astype(BF16).astype(F32)
    slow = slow_ref[...] * (-gate_const)

    def step(j, carry):
        state, decay = carry
        at = pl.ds(pl.multiple_of(j * SUB, SUB), SUB)
        recur = jax.nn.sigmoid(pre_ref[at, :cols])
        inject = jax.nn.sigmoid(pre_ref[at, cols:])
        log_decay = recur * slow + wide_ref[at, :]
        a = jnp.exp(log_decay)
        u = 2.0 * log_decay
        series = 1.0 / 40320.0
        for c in (5040.0, 720.0, 120.0, 24.0, 6.0, 2.0, 1.0):
            series = series * u + 1.0 / c
        gone = jnp.where(u > -0.5, -u * series, 1.0 - a * a)
        drive = jnp.sqrt(gone) * inject * xf_ref[at, :]
        state = a * state + drive
        decay = a * decay
        opening = jax.nn.gelu(bg_ref[at, :])
        return state, decay, state * opening, decay * opening

    unroll = 4 if steps % 4 == 0 else 2

    def several(i, carry):
        at = pl.ds(pl.multiple_of(i * unroll * SUB, unroll * SUB), unroll * SUB)
        locs, accs = [], []
        for n in range(unroll):
            *carry, loc, acc = step(i * unroll + n, carry)
            locs.append(loc)
            accs.append(acc)
        body_ref[0, at, :] = jnp.concatenate(locs, axis=0).astype(BF16)
        body_ref[1, at, :] = jnp.concatenate(accs, axis=0).astype(BF16)
        return tuple(carry)

    state, decay = lax.fori_loop(
        0,
        steps // unroll,
        several,
        (jnp.zeros((SUB, cols), F32), jnp.ones((SUB, cols), F32)),
    )
    for d in (1, 2, 4):
        behind_state = pltpu.roll(state, d, 0)
        behind_decay = pltpu.roll(decay, d, 0)
        state = jnp.where(sub >= d, decay * behind_state + state, state)
        decay = jnp.where(sub >= d, decay * behind_decay, decay)
    edge_ref[:SUB, :] = jnp.where(sub == 0, 0.0, pltpu.roll(state, 1, 0))
    edge_ref[SUB : 2 * SUB, :] = jnp.where(sub == 0, 1.0, pltpu.roll(decay, 1, 0))
    edge_ref[2 * SUB :, :] = jnp.where(
        sub == 0,
        jnp.broadcast_to(decay[SUB - 1 :], sub.shape),
        jnp.broadcast_to(state[SUB - 1 :], sub.shape),
    )


def chain(decay, state, part):
    return part[0:1] * decay, part[0:1] * state + part[1:2]


def choose(parts, index):
    picked = parts[0]
    for k in range(1, len(parts)):
        picked = jnp.where(index == k, parts[k], picked)
    return picked


def ends_of(edge_refs):
    return [
        r[i, 2 * SUB : 2 * SUB + 2] for r in edge_refs for i in range(r.shape[0])
    ]


def total_kernel(arrays, place_ref, *refs):
    tots, out_ref = ends_of(refs[:arrays]), refs[arrays]
    me = place_ref[0]
    decay = jnp.ones((1, out_ref.shape[1]), F32)
    state = jnp.zeros((1, out_ref.shape[1]), F32)
    for b in range(len(tots)):
        decay, state = chain(decay, state, choose(tots, me ^ b))
    out_ref[0:1, :] = decay
    out_ref[1:2, :] = state


def entering(total):
    here = lax.axis_index("ep")
    group = total
    before = jnp.concatenate([jnp.ones_like(total[0:1]), jnp.zeros_like(total[1:2])], axis=0)
    bit = 1
    while bit < lax.axis_size("ep"):
        other = swap(group, "ep", bit)
        late = (here & bit) != 0
        before = jnp.where(late, join(other, before), before)
        group = jnp.where(late, join(other, group), join(group, other))
        bit *= 2
    return before[1:2]


def join(earlier, later):
    decay, state = chain(earlier[0:1], earlier[1:2], later)
    return jnp.concatenate([decay, state], axis=0)


def out_kernel(arrays, ks, place_ref, entry_ref, *refs):
    edges = refs[:arrays]
    tots = ends_of(edges)
    prefs = [r[i, : 2 * SUB] for r in edges for i in range(r.shape[0])]
    rest = refs[arrays:]
    outs = rest[len(rest) - len(ks) :]
    w_ref = rest[len(rest) - len(ks) - 1]
    bodies = [(r, i) for r in rest[: len(rest) - len(ks) - 1] for i in range(r.shape[0])]
    me = place_ref[0]
    cols = w_ref.shape[0]
    entry = entry_ref[...]
    entries = []
    decay = jnp.ones((1, cols), F32)
    for b in range(len(tots)):
        entries.append(entry)
        decay, entry = chain(decay, entry, choose(tots, me ^ b))
    rows = outs[0].shape[0]
    t = lax.broadcasted_iota(jnp.int32, (rows, rows), 0)
    r = lax.broadcasted_iota(jnp.int32, (rows, rows), 1)
    order = (t == (r % SUB) * (rows // SUB) + r // SUB).astype(F32).astype(BF16)
    for n, k in enumerate(ks):
        carried = choose(entries, me ^ k)
        lift = prefs[k][:SUB] + prefs[k][SUB:] * carried
        lift = jnp.broadcast_to(lift[None], (rows // SUB, SUB, cols)).reshape(rows, cols)
        ref, i = bodies[n]
        mixed = (ref[i, 0].astype(F32) + ref[i, 1].astype(F32) * lift).astype(BF16)
        mixed = dotf(order, mixed).astype(BF16)
        outs[n][...] = dotf(mixed, w_ref[...]).astype(outs[n].dtype)


def add_kernel(a_ref, b_ref, out_ref):
    out_ref[...] = (a_ref[...].astype(F32) + b_ref[...].astype(F32)).astype(out_ref.dtype)


def slots_of(ids, flip, room, experts, axis):
    tokens = ids.shape[1 - axis]
    picks = ids.shape[axis]
    shape = (experts, tokens) if axis == 0 else (tokens, experts)
    number = lax.broadcasted_iota(jnp.int32, shape, axis)
    cut = [ids[k : k + 1, :] if axis == 0 else ids[:, k : k + 1] for k in range(picks)]
    hot = [(c == number).astype(F32) for c in cut]
    r = lax.broadcasted_iota(jnp.int32, (tokens, tokens), 0)
    c = lax.broadcasted_iota(jnp.int32, (tokens, tokens), 1)
    every = functools.reduce(lambda a, b: a + b, hot).astype(BF16)
    if axis == 0:
        seen = dotf(every, (r < c).astype(F32).astype(BF16))
    else:
        seen = dotf((c < r).astype(F32).astype(BF16), every)
    return [
        (c ^ flip) * room + jnp.sum(h * seen, axis=axis, keepdims=True).astype(jnp.int32)
        for c, h in zip(cut, hot)
    ]


def dispatch_kernel(experts, room, place_ref, x_ref, gain_ref, ids_ref, *outs):
    values = x_ref[...].astype(F32)
    inv = lax.rsqrt(jnp.mean(values * values, axis=-1, keepdims=True) + epsilon)
    normed = (values * inv * gain_ref[...][None, :].astype(F32)).astype(BF16)
    slots = slots_of(ids_ref[...], place_ref[2], room, experts, 0)
    number = lax.broadcasted_iota(jnp.int32, (experts * room, values.shape[0]), 0)
    table = functools.reduce(jnp.logical_or, [number == s for s in slots])
    rows = dotf(table.astype(F32).astype(BF16), normed).astype(BF16)
    at = 0
    for out in outs:
        out[...] = rows[at : at + out.shape[0]]
        at += out.shape[0]


def combine_kernel(experts, room, place_ref, ids_ref, weight_ref, *refs):
    out_ref = refs[-1]
    slots = slots_of(ids_ref[...], place_ref[2], room, experts, 1)
    number = lax.broadcasted_iota(jnp.int32, (out_ref.shape[0], experts * room), 1)
    table = jnp.zeros(number.shape, F32)
    for k, s in enumerate(slots):
        table = jnp.where(number == s, weight_ref[:, k : k + 1], table)
    high, middle, small = split3(table)
    value = stacked(refs[:-1])
    done = dotf(high, value) + (dotf(middle, value) + dotf(small, value))
    out_ref[...] = done.astype(BF16)


def exchange_all(pieces):
    if len(pieces) == 1:
        return [exchange(pieces[0], "ep")]
    got = {0: pieces[0]}
    for m in list(range(2, len(pieces))) + [1]:
        got[m] = swap(pieces[m], "ep", m)
    return [got[m] for m in range(len(pieces))]


def stacked(refs):
    values = [r[...] for r in refs]
    return values[0] if len(values) == 1 else jnp.concatenate(values, axis=0)


def hidden_kernel(pieces, n, *refs):
    x = stacked(refs[:pieces])
    refs = refs[pieces:]
    out_ref = refs[2 * n]
    span = refs[0].shape[1]
    for i in range(n):
        gate = dotf(x, refs[i][...])
        up = dotf(x, refs[n + i][...])
        out_ref[:, i * span : (i + 1) * span] = (jax.nn.silu(gate) * up).astype(BF16)


def down_kernel(n, h_ref, *refs):
    parts, outs = refs[:n], refs[n:]
    span = parts[0].shape[0]
    total = dotf(h_ref[:, :span], parts[0][...])
    for i in range(1, n):
        total = total + dotf(h_ref[:, i * span : (i + 1) * span], parts[i][...])
    at = 0
    for out in outs:
        out[...] = total[at : at + out.shape[0]].astype(BF16)
        at += out.shape[0]


def body(
    mix_tokens,
    mix_gain,
    w_branch,
    w_gate_branch,
    conv_taps,
    recur_gate_w,
    inject_gate_w,
    decay_logit,
    decay_kick,
    w_mix_out,
    moe_tokens,
    moe_gain,
    expert_ids,
    route_weight,
    expert_gate_w,
    expert_up_w,
    expert_down_w,
):
    shape = jax.ShapeDtypeStruct
    me = lax.axis_index("tp")
    here = lax.axis_index("ep")
    count = lax.axis_size("tp")
    ep_size = lax.axis_size("ep")
    direct = 1 < ep_size <= 8
    place = jnp.stack([me, here, here if direct else 0 * here]).astype(jnp.int32)
    rows, width = mix_tokens.shape
    cols = w_branch.shape[1]
    taps_count = conv_taps.shape[0]
    steps = rows // SUB
    half = max(count // 2, 1)

    before = from_behind(mix_tokens[rows - 2 * SUB :], "ep", 1)

    local_rows, top_count = expert_ids.shape
    slots_total = 2 * local_rows * top_count
    room = slots_total // ep_size
    pieces = ep_size if direct else 1
    outgoing = call(
        functools.partial(dispatch_kernel, ep_size, room),
        tuple(shape((slots_total // pieces, width), BF16) for _ in range(pieces)),
        2 * local_rows * slots_total * width,
        place,
        moe_tokens,
        moe_gain,
        expert_ids.T,
        smem=(0,),
        alone=True,
    )
    arrived = exchange_all(outgoing)
    gate_parts = spread(expert_gate_w[0])
    up_parts = spread(expert_up_w[0])
    down = expert_down_w[0]
    first = width * 5 // 8 // 128 * 128
    spans = (first, width - first)
    down_parts = [spread(down[:, sum(spans[:i]) : sum(spans[: i + 1])]) for i in range(len(spans))]

    mixer_in, tail = call(
        norm_kernel,
        (shape((rows, width), BF16), shape((4 * SUB, width), BF16)),
        2 * rows * rows * width,
        mix_tokens,
        before,
        mix_gain,
        alone=True,
    )
    tails = spread(tail)
    blocks = spread(mixer_in)

    head_count, head_dim, _ = recur_gate_w.shape
    group = 256 if cols % 256 == 0 and 256 % head_dim == 0 else cols
    gates = call(
        gates_kernel,
        shape((cols // group, group, 2 * group), BF16),
        4 * cols * group * head_dim,
        recur_gate_w.reshape(cols, head_dim),
        inject_gate_w.reshape(cols, head_dim),
    )
    slowness = jax.nn.softplus(-decay_logit)[None, :]
    kick = decay_kick.reshape(count, SUB, steps, head_count).swapaxes(1, 2)
    kick = kick.reshape(count, rows, head_count)
    parts = {}

    def run_blocks(ks):
        made = call(
            functools.partial(block_kernel, taps_count, ks),
            (
                shape((len(ks), 2, rows, cols), BF16),
                shape((len(ks), 3 * SUB, cols), F32),
            ),
            2 * len(ks) * rows * cols * (2 * width + 2 * group),
            place,
            kick,
            w_branch,
            w_gate_branch,
            conv_taps,
            gates,
            slowness,
            *tails,
            *[blocks[k] for k in ks],
            scratch=(
                pltpu.VMEM((rows + (taps_count - 1) * SUB, cols), F32),
                pltpu.VMEM((rows, cols), F32),
                pltpu.VMEM((rows, 2 * cols), F32),
                pltpu.VMEM((rows, cols), F32),
            ),
            smem=(0,),
        )
        parts[ks] = made

    run_blocks(tuple(range(half)))
    for k in range(half, count):
        run_blocks((k,))
    groups = sorted(parts)
    edges = [parts[ks][1] for ks in groups]
    ends = call(
        functools.partial(total_kernel, len(groups)),
        shape((2, cols), F32),
        1000,
        place,
        *edges,
        smem=(0,),
    )
    entry = entering(ends)

    def project(ks):
        return call(
            functools.partial(out_kernel, len(groups), ks),
            tuple(shape((rows, width), BF16) for _ in ks),
            2 * len(ks) * rows * cols * width,
            place,
            entry,
            *edges,
            *[parts[g][0] for g in groups if set(g) <= set(ks)],
            w_mix_out,
            smem=(0,),
        )

    made = dict(zip(range(half, count), project(tuple(range(half, count)))))
    made.update(zip(range(half), project(tuple(range(half)))))
    bit = 1
    while bit < count:
        for k in sorted((k for k in made if not k & bit), reverse=True):
            last = k == 0 and 2 * bit == count
            made[k] = call(
                add_kernel,
                shape((rows, width), BF16 if k or last else F32),
                rows * width,
                made[k],
                swap(made.pop(k ^ bit), "tp", bit),
            )
        bit *= 2
    mixer_out = made[0].astype(BF16)

    hidden = call(
        functools.partial(hidden_kernel, pieces, count),
        shape((slots_total, count * gate_parts[0].shape[1]), BF16),
        4 * count * slots_total * width * gate_parts[0].shape[1],
        *arrived,
        *gate_parts,
        *up_parts,
    )
    returned = []
    for i, span in enumerate(spans):
        done = call(
            functools.partial(down_kernel, count),
            tuple(shape((slots_total // pieces, span), BF16) for _ in range(pieces)),
            2 * slots_total * span * count * down.shape[0],
            hidden,
            *down_parts[i],
        )
        returned.append(
            call(
                functools.partial(combine_kernel, ep_size, room),
                shape((local_rows, span), BF16),
                6 * local_rows * slots_total * span,
                place,
                expert_ids,
                route_weight,
                *exchange_all(done),
                smem=(0,),
            )
        )
    expert_out = jnp.concatenate(returned, axis=1)
    return (mixer_out, expert_out)


def solution(mesh):
    placed = (
        P(("ep", "tp"), None),
        P(),
        P(None, "tp"),
        P(None, "tp"),
        P(None, "tp"),
        P("tp", None, None),
        P("tp", None, None),
        P("tp"),
        P("ep", "tp"),
        P("tp", None),
        P(("ep", "tp"), None),
        P(),
        P(("ep", "tp"), None),
        P(("ep", "tp"), None),
        P("ep", None, "tp"),
        P("ep", None, "tp"),
        P("ep", "tp", None),
    )
    return jax.shard_map(
        body,
        mesh=mesh,
        in_specs=placed,
        out_specs=(P(("ep", "tp"), None), P(("ep", "tp"), None)),
        check_vma=False,
    )
```

```python
import functools
import math

import jax
import jax.numpy as jnp
from jax import lax
from jax.experimental import pallas as pl
from jax.experimental.pallas import tpu as pltpu
from jax.sharding import PartitionSpec as P


epsilon = 1e-06
gate_const = 8.0
SUB = 8
SPARE = 6
COPIES = 4
F32 = jnp.float32
BF16 = jnp.bfloat16


def dotf(a, b):
    return jnp.dot(a, b, preferred_element_type=F32)


def swap(block, axis, bit):
    size = lax.axis_size(axis)
    return lax.ppermute(block, axis, [(i, i ^ bit) for i in range(size)])


def from_behind(block, axes):
    size = math.prod(lax.axis_size(a) for a in axes)
    return lax.ppermute(block, axes, [(i, i + 1) for i in range(size - 1)])


def exchange(block, axis):
    return lax.all_to_all(block, axis, split_axis=0, concat_axis=0, tiled=True)


def tp_bits():
    size, bits = lax.axis_size("tp"), []
    while size > 1:
        size //= 2
        bits.append(size)
    return bits


def spread(block):
    held = {0: block}
    for bit in tp_bits():
        held.update({k ^ bit: swap(v, "tp", bit) for k, v in list(held.items())})
    return [held[k] for k in range(len(held))]


def cost(flops, moved, transcendentals=0):
    return pl.CostEstimate(flops=flops, bytes_accessed=moved, transcendentals=transcendentals)


def call(
    kernel, outs, flops, *args, scratch=(), smem=(), grid=None, maps=(), out_maps=None, far=(), alone=False,
    stay=False, far_out=False
):
    sizes = [a.size * a.dtype.itemsize for a in args]
    sizes += [o.size * o.dtype.itemsize for o in jax.tree.leaves(outs)]
    moved = sum(sizes)
    if not alone:
        held = moved + sum(math.prod(v.shape) * v.dtype.itemsize for v in scratch if hasattr(v.dtype, "itemsize"))

    def spec(i, a):
        if i in smem:
            return pl.BlockSpec(memory_space=pltpu.SMEM)
        if i in far:
            return pl.BlockSpec(memory_space=pl.ANY)
        if grid is None:
            return pl.BlockSpec(memory_space=pltpu.VMEM)
        if i in maps:
            return pl.BlockSpec(*maps[i])
        return pl.BlockSpec(a.shape, lambda n, rank=a.ndim: (0,) * rank)

    return pl.pallas_call(
        kernel,
        out_shape=jax.tree.map(lambda o: pltpu.VMEM(o.shape, o.dtype), outs) if stay else outs,
        grid=() if grid is None else (grid,),
        in_specs=[spec(i, a) for i, a in enumerate(args)],
        out_specs=jax.tree.map(
            lambda o: pl.BlockSpec(*out_maps)
            if grid
            else pl.BlockSpec(memory_space=pl.ANY if far_out else pltpu.VMEM),
            outs,
        ),
        scratch_shapes=list(scratch),
        cost_estimate=cost(flops, moved),
        compiler_params=pltpu.CompilerParams(
            vmem_limit_bytes=None if grid or alone else held + (SPARE << 20)
        ),
    )(*args)


def normed_rows(x_ref, gain_ref):
    values = x_ref[...].astype(F32)
    inv = lax.rsqrt(jnp.mean(values * values, axis=-1, keepdims=True) + epsilon)
    return (values * inv * gain_ref[...][None, :].astype(F32)).astype(BF16)


def norm_kernel(x_ref, gain_ref, out_ref):
    normed = normed_rows(x_ref, gain_ref)
    out_ref[...] = dotf(time_order(x_ref.shape[0]), normed).astype(BF16)


def time_order(rows, back=False):
    steps = rows // SUB
    r = lax.broadcasted_iota(jnp.int32, (rows, rows), 1 if back else 0)
    t = lax.broadcasted_iota(jnp.int32, (rows, rows), 0 if back else 1)
    return (t == (r % SUB) * steps + r // SUB).astype(F32).astype(BF16)


def stage_kernel(from_ref, to_ref, sem):
    copy = pltpu.make_async_copy(from_ref, to_ref, sem)
    copy.start()
    copy.wait()


def prepare_kernel(spans, down_ref, recur_ref, inject_ref, gates_ref, *outs):
    at = 0
    for out, span in zip(outs, spans):
        out[...] = down_ref[:, at : at + span]
        at += span
    gates_kernel(recur_ref, inject_ref, gates_ref)


def split3(values):
    high = values.astype(BF16)
    rest = values - high.astype(F32)
    middle = rest.astype(BF16)
    return high, middle, (rest - middle.astype(F32)).astype(BF16)


def gates_kernel(recur_ref, inject_ref, out_ref):
    groups, width, _ = out_ref.shape
    head = recur_ref.shape[1]
    j = lax.broadcasted_iota(jnp.int32, (head, width), 0)
    c = lax.broadcasted_iota(jnp.int32, (head, width), 1)
    repeat = (c % head == j).astype(F32).astype(BF16)
    r = lax.broadcasted_iota(jnp.int32, (width, width), 0)
    c = lax.broadcasted_iota(jnp.int32, (width, width), 1)
    same = r // head == c // head
    for g in range(groups):
        for i, ref in enumerate((recur_ref, inject_ref)):
            wide = dotf(ref[g * width : (g + 1) * width, :], repeat)
            out_ref[g, :, i * width : (i + 1) * width] = jnp.where(same, wide, 0.0).astype(BF16)


def block_kernel(taps_count, count, ks, held, place_ref, *refs):
    edges, refs = refs[:held], refs[held:]
    n = len(ks)
    kick_ref, gain_ref, wb_ref, wg_ref, taps_ref, gates_ref, slow_ref = refs[:7]
    leads, xs, refs = refs[7 : 7 + n], refs[7 + n : 7 + 2 * n], refs[7 + 2 * n :]
    body_ref, edge_ref = refs[:2]
    scratch = refs[len(refs) - 4 :]
    me = place_ref[0]
    for i, k in enumerate(ks):
        rows = xs[i].shape[0]
        one_block(
            taps_count,
            xs[i],
            normed_rows(leads[i], gain_ref),
            kick_ref[:, pl.ds((me ^ k) * rows, rows)],
            wb_ref,
            wg_ref,
            taps_ref,
            gates_ref,
            slow_ref,
            body_ref.at[i],
            edge_ref.at[i],
            *scratch,
        )
    if held:
        decay = jnp.ones((1, edge_ref.shape[2]), F32)
        state = jnp.zeros((1, edge_ref.shape[2]), F32)
        tots = ends_of((*edges, edge_ref))
        for b in range(count):
            decay, state = chain(decay, state, choose(tots, me ^ b))
        total_ref = refs[2]
        total_ref[0:1, :] = decay
        total_ref[1:2, :] = state


def one_block(
    taps_count,
    x_ref,
    lead_rows,
    kicks,
    wb_ref,
    wg_ref,
    taps_ref,
    gates_ref,
    slow_ref,
    body_ref,
    edge_ref,
    xf_ref,
    bg_ref,
    pre_ref,
    wide_ref,
):
    _, rows, cols = body_ref.shape
    steps = rows // SUB
    lead = taps_count - 1
    x = x_ref[...]
    bt = dotf(lead_rows, wb_ref[...]).astype(BF16).astype(F32)
    bt = bt[bt.shape[0] - lead :]
    xf_ref[lead * SUB :, :] = dotf(x, wb_ref[...]).astype(BF16).astype(F32)
    sub = lax.broadcasted_iota(jnp.int32, (SUB, cols), 0)
    for m in range(lead):
        at = rows + m * SUB
        shifted = pltpu.roll(xf_ref[at : at + SUB, :], 1, 0)
        xf_ref[m * SUB : (m + 1) * SUB, :] = jnp.where(sub == 0, bt[m : m + 1], shifted)
    taps = taps_ref[...].astype(F32)
    conv = taps[0:1] * xf_ref[:rows, :]
    for k in range(1, taps_count):
        conv = conv + taps[k : k + 1] * xf_ref[k * SUB : k * SUB + rows, :]
    xf_ref[:rows, :] = conv
    low = conv.astype(BF16)
    width = gates_ref.shape[1]
    for g in range(cols // width):
        pre = dotf(low[:, g * width : (g + 1) * width], gates_ref[g])
        pre_ref[:, g * width : (g + 1) * width] = pre[:, :width]
        pre_ref[:, cols + g * width : cols + (g + 1) * width] = pre[:, width:]
    heads = kicks.shape[0]
    h = lax.broadcasted_iota(jnp.int32, (heads, cols), 0)
    c = lax.broadcasted_iota(jnp.int32, (heads, cols), 1)
    widen = (c // (cols // heads) == h).astype(F32).astype(BF16)
    order = time_order(rows)
    high, middle, small = [
        dotf(dotf(order, part).astype(BF16), widen) for part in split3(jnp.transpose(kicks))
    ]
    wide_ref[...] = high + (middle + small)
    bg_ref[...] = dotf(x, wg_ref[...]).astype(BF16).astype(F32)
    slow = slow_ref[...] * (-gate_const)

    def step(j, carry):
        state, decay = carry
        at = pl.ds(pl.multiple_of(j * SUB, SUB), SUB)
        recur = jax.nn.sigmoid(pre_ref[at, :cols])
        inject = jax.nn.sigmoid(pre_ref[at, cols:])
        log_decay = recur * slow + wide_ref[at, :]
        a = jnp.exp(log_decay)
        u = 2.0 * log_decay
        series = 1.0 / 40320.0
        for c in (5040.0, 720.0, 120.0, 24.0, 6.0, 2.0, 1.0):
            series = series * u + 1.0 / c
        gone = jnp.where(u > -0.5, -u * series, 1.0 - a * a)
        drive = jnp.sqrt(gone) * inject * xf_ref[at, :]
        state = a * state + drive
        decay = a * decay
        opening = jax.nn.gelu(bg_ref[at, :])
        return state, decay, state * opening, decay * opening

    unroll = 4 if steps % 4 == 0 else 2

    def several(i, carry):
        at = pl.ds(pl.multiple_of(i * unroll * SUB, unroll * SUB), unroll * SUB)
        locs, accs = [], []
        for n in range(unroll):
            *carry, loc, acc = step(i * unroll + n, carry)
            locs.append(loc)
            accs.append(acc)
        body_ref[0, at, :] = jnp.concatenate(locs, axis=0).astype(BF16)
        body_ref[1, at, :] = jnp.concatenate(accs, axis=0).astype(BF16)
        return tuple(carry)

    state, decay = lax.fori_loop(
        0,
        steps // unroll,
        several,
        (jnp.zeros((SUB, cols), F32), jnp.ones((SUB, cols), F32)),
    )
    for d in (1, 2, 4):
        behind_state = pltpu.roll(state, d, 0)
        behind_decay = pltpu.roll(decay, d, 0)
        state = jnp.where(sub >= d, decay * behind_state + state, state)
        decay = jnp.where(sub >= d, decay * behind_decay, decay)
    edge_ref[:SUB, :] = jnp.where(sub == 0, 0.0, pltpu.roll(state, 1, 0))
    edge_ref[SUB : 2 * SUB, :] = jnp.where(sub == 0, 1.0, pltpu.roll(decay, 1, 0))
    edge_ref[2 * SUB :, :] = jnp.where(
        sub == 0,
        jnp.broadcast_to(decay[SUB - 1 :], sub.shape),
        jnp.broadcast_to(state[SUB - 1 :], sub.shape),
    )


def chain(decay, state, part):
    return part[0:1] * decay, part[0:1] * state + part[1:2]


def choose(parts, index):
    picked = parts[0]
    for k in range(1, len(parts)):
        picked = jnp.where(index == k, parts[k], picked)
    return picked


def ends_of(edge_refs):
    return [
        r[i, 2 * SUB : 2 * SUB + 2] for r in edge_refs for i in range(r.shape[0])
    ]


def quad_kernel(place_ref, *refs):
    members, (group_ref, before_ref) = [r[...] for r in refs[:-2]], refs[-2:]
    mine = place_ref[1] & (len(members) - 1)
    unit = lax.broadcasted_iota(jnp.int32, group_ref.shape, 0) == 0
    group = before = jnp.where(unit, 1.0, 0.0)
    for b in range(len(members)):
        other = choose(members, mine ^ b)
        group = join(group, other)
        before = jnp.where(b < mine, group, before)
    group_ref[...] = group
    before_ref[...] = before


def entering(place, total):
    size = lax.axis_size("ep")
    here = lax.axis_index("ep")
    first = min(size, 4)
    pair = jax.ShapeDtypeStruct(total.shape, F32)
    members = [total] + [swap(total, "ep", m) for m in range(1, first)]
    group, before = call(quad_kernel, (pair, pair), 1000, place, *members, smem=(0,))
    bit = first
    other = before
    while bit < size:
        other = swap(group, "ep", bit)
        late = (here & bit) != 0
        bit *= 2
        if bit < size:
            before = jnp.where(late, join(other, before), before)
            group = jnp.where(late, join(other, group), join(group, other))
    return before, other


def join(earlier, later):
    decay, state = chain(earlier[0:1], earlier[1:2], later)
    first = lax.broadcasted_iota(jnp.int32, later.shape, 0) == 0
    return jnp.where(first, decay, state)


def out_kernel(arrays, ks, place_ref, before_ref, other_ref, *refs):
    edges = refs[:arrays]
    tots = ends_of(edges)
    prefs = [r[i, : 2 * SUB] for r in edges for i in range(r.shape[0])]
    n = len(ks)
    given, (mixed_ref, made_ref, sems) = refs[arrays:-3], refs[-3:]
    given, outs = given[: len(given) - n], given[len(given) - n :]
    bodies = [r.at[i] for r in given[:-1] for i in range(r.shape[0])]
    wide_ref = given[-1]
    mix_blocks(ks, place_ref, before_ref, other_ref, tots, prefs, bodies, mixed_ref)
    stores = []
    cut = wide_ref.shape[1] // COPIES
    for i in range(n):
        for c in range(COPIES):
            at = slice(c * cut, (c + 1) * cut)
            made_ref[i, :, at] = dotf(mixed_ref[i], wide_ref[:, at]).astype(BF16)
            stores.append(
                pltpu.make_async_copy(
                    made_ref.at[i, :, at], outs[i].at[:, at], sems.at[len(stores)]
                )
            )
            stores[-1].start()
    for copy in stores:
        copy.wait()


def mix_blocks(ks, place_ref, before_ref, other_ref, tots, prefs, bodies, mixed_ref):
    me = place_ref[0]
    _, rows, cols = mixed_ref.shape
    before = before_ref[...]
    entry = jnp.where(place_ref[3] != 0, join(other_ref[...], before), before)[1:2]
    entries = []
    decay = jnp.ones((1, cols), F32)
    for b in range(len(tots)):
        entries.append(entry)
        decay, entry = chain(decay, entry, choose(tots, me ^ b))
    order = time_order(rows, back=True)
    for n, k in enumerate(ks):
        carried = choose(entries, me ^ k)
        lift = prefs[k][:SUB] + prefs[k][SUB:] * carried
        lift = jnp.broadcast_to(lift[None], (rows // SUB, SUB, cols)).reshape(rows, cols)
        mixed = (bodies[n][0].astype(F32) + bodies[n][1].astype(F32) * lift).astype(BF16)
        mixed_ref[n] = dotf(order, mixed).astype(BF16)


def add_kernel(a_ref, b_ref, out_ref):
    out_ref[...] = (a_ref[...].astype(F32) + b_ref[...].astype(F32)).astype(out_ref.dtype)


def slots_of(ids, flip, room, experts, axis):
    tokens = ids.shape[1 - axis]
    picks = ids.shape[axis]
    shape = (experts, tokens) if axis == 0 else (tokens, experts)
    number = lax.broadcasted_iota(jnp.int32, shape, axis)
    cut = [ids[k : k + 1, :] if axis == 0 else ids[:, k : k + 1] for k in range(picks)]
    hot = [(c == number).astype(F32) for c in cut]
    r = lax.broadcasted_iota(jnp.int32, (tokens, tokens), 0)
    c = lax.broadcasted_iota(jnp.int32, (tokens, tokens), 1)
    every = functools.reduce(lambda a, b: a + b, hot).astype(BF16)
    if axis == 0:
        seen = dotf(every, (r < c).astype(F32).astype(BF16))
    else:
        seen = dotf((c < r).astype(F32).astype(BF16), every)
    return [
        (c ^ flip) * room + jnp.sum(h * seen, axis=axis, keepdims=True).astype(jnp.int32)
        for c, h in zip(cut, hot)
    ]


def dispatch_kernel(experts, room, place_ref, x_ref, gain_ref, ids_ref, *outs):
    values = x_ref[...].astype(F32)
    inv = lax.rsqrt(jnp.mean(values * values, axis=-1, keepdims=True) + epsilon)
    normed = (values * inv * gain_ref[...][None, :].astype(F32)).astype(BF16)
    slots = slots_of(ids_ref[...], place_ref[2], room, experts, 0)
    number = lax.broadcasted_iota(jnp.int32, (experts * room, values.shape[0]), 0)
    table = functools.reduce(jnp.logical_or, [number == s for s in slots])
    rows = dotf(table.astype(F32).astype(BF16), normed).astype(BF16)
    at = 0
    for out in outs:
        out[...] = rows[at : at + out.shape[0]]
        at += out.shape[0]


def combine_kernel(experts, room, held, place_ref, ids_ref, weight_ref, *refs):
    parts, out_ref = refs[held:-1], refs[-1]
    slots = slots_of(ids_ref[...], place_ref[2], room, experts, 1)
    number = lax.broadcasted_iota(jnp.int32, (out_ref.shape[0], experts * room), 1)
    table = jnp.zeros(number.shape, F32)
    for k, s in enumerate(slots):
        table = jnp.where(number == s, weight_ref[:, k : k + 1], table)
    high, middle, small = split3(table)
    value = stacked(parts)
    done = dotf(high, value) + (dotf(middle, value) + dotf(small, value))
    at = 0
    for ref in refs[:held]:
        out_ref[:, at : at + ref.shape[1]] = ref[...]
        at += ref.shape[1]
    out_ref[:, at:] = done.astype(BF16)


def exchange_all(pieces):
    if len(pieces) == 1:
        return [exchange(pieces[0], "ep")]
    got = {0: pieces[0]}
    for m in list(range(2, len(pieces))) + [1]:
        got[m] = swap(pieces[m], "ep", m)
    return [got[m] for m in range(len(pieces))]


def stacked(refs):
    values = [r[...] for r in refs]
    return values[0] if len(values) == 1 else jnp.concatenate(values, axis=0)


def hidden_kernel(pieces, n, *refs):
    x = stacked(refs[:pieces])
    refs = refs[pieces:]
    out_ref = refs[2 * n]
    span = refs[0].shape[1]
    for i in range(n):
        gate = dotf(x, refs[i][...])
        up = dotf(x, refs[n + i][...])
        out_ref[:, i * span : (i + 1) * span] = (jax.nn.silu(gate) * up).astype(BF16)


def down_kernel(n, h_ref, *refs):
    parts, outs = refs[:n], refs[n:]
    span = parts[0].shape[0]
    total = dotf(h_ref[:, :span], parts[0][...])
    for i in range(1, n):
        total = total + dotf(h_ref[:, i * span : (i + 1) * span], parts[i][...])
    at = 0
    for out in outs:
        out[...] = total[at : at + out.shape[0]].astype(BF16)
        at += out.shape[0]


def body(
    mix_tokens,
    mix_gain,
    w_branch,
    w_gate_branch,
    conv_taps,
    recur_gate_w,
    inject_gate_w,
    decay_logit,
    decay_kick,
    w_mix_out,
    moe_tokens,
    moe_gain,
    expert_ids,
    route_weight,
    expert_gate_w,
    expert_up_w,
    expert_down_w,
):
    shape = jax.ShapeDtypeStruct
    me = lax.axis_index("tp")
    here = lax.axis_index("ep")
    count = lax.axis_size("tp")
    ep_size = lax.axis_size("ep")
    direct = 1 < ep_size <= 8
    late = here & (ep_size // 2) if ep_size > 4 else 0 * here
    place = jnp.stack([me, here, here if direct else 0 * here, late]).astype(jnp.int32)
    rows, width = mix_tokens.shape
    cols = w_branch.shape[1]
    taps_count = conv_taps.shape[0]
    half = max(count // 2, 1)

    lead = from_behind(mix_tokens[rows - 2 * SUB :], ("ep", "tp"))

    local_rows, top_count = expert_ids.shape
    slots_total = 2 * local_rows * top_count
    room = slots_total // ep_size
    pieces = ep_size if direct else 1
    outgoing = call(
        functools.partial(dispatch_kernel, ep_size, room),
        tuple(shape((slots_total // pieces, width), BF16) for _ in range(pieces)),
        2 * local_rows * slots_total * width,
        place,
        moe_tokens,
        moe_gain,
        expert_ids.T,
        smem=(0,),
        alone=True,
    )
    arrived = exchange_all(outgoing)
    gate_parts = spread(expert_gate_w[0])
    up_parts = spread(expert_up_w[0])
    down = expert_down_w[0]
    first = width * 5 // 8 // 128 * 128
    spans = (first, width - first)
    _, head_dim, _ = recur_gate_w.shape
    group = 256 if cols % 256 == 0 and 256 % head_dim == 0 else cols
    gates, *down_cut = call(
        functools.partial(prepare_kernel, spans),
        (
            shape((cols // group, group, 2 * group), BF16),
            *[shape((down.shape[0], span), BF16) for span in spans],
        ),
        4 * cols * group * head_dim,
        down,
        recur_gate_w.reshape(cols, head_dim),
        inject_gate_w.reshape(cols, head_dim),
    )
    down_parts = [spread(part) for part in down_cut]

    mixer_in = call(
        norm_kernel,
        shape((rows, width), BF16),
        2 * rows * rows * width,
        mix_tokens,
        mix_gain,
        alone=True,
    )
    leads = spread(lead)
    blocks = spread(mixer_in)

    slowness = jax.nn.softplus(-decay_logit)[None, :]
    kick = decay_kick.T
    parts = {}

    def run_blocks(ks):
        outs = (
            shape((len(ks), 2, rows, cols), BF16),
            shape((len(ks), 3 * SUB, cols), F32),
        )
        edges = []
        if ks[-1] == count - 1:
            outs += (shape((2, cols), F32),)
            edges = [parts[g][1] for g in sorted(parts)]
        made = call(
            functools.partial(block_kernel, taps_count, count, ks, len(edges)),
            outs,
            2 * len(ks) * rows * cols * (2 * width + 2 * group),
            place,
            *edges,
            kick,
            mix_gain,
            w_branch,
            w_gate_branch,
            conv_taps,
            gates,
            slowness,
            *[leads[k] for k in ks],
            *[blocks[k] for k in ks],
            scratch=(
                pltpu.VMEM((rows + (taps_count - 1) * SUB, cols), F32),
                pltpu.VMEM((rows, cols), F32),
                pltpu.VMEM((rows, 2 * cols), F32),
                pltpu.VMEM((rows, cols), F32),
            ),
            smem=(0,),
            stay=True,
        )
        parts[ks] = made

    run_blocks(tuple(range(half)))
    for k in range(half, count):
        run_blocks((k,))
    groups = sorted(parts)
    edges = [parts[ks][1] for ks in groups]
    entry = entering(place, parts[groups[-1]][2])

    wide = call(
        stage_kernel,
        shape(w_mix_out.shape, BF16),
        1000,
        w_mix_out,
        scratch=(pltpu.SemaphoreType.DMA(()),),
        far=(0,),
        stay=True,
    )

    def project(ks):
        args = [
            place,
            *entry,
            *edges,
            *[parts[g][0] for g in groups if set(g) <= set(ks)],
            wide,
        ]
        return call(
            functools.partial(out_kernel, len(groups), ks),
            tuple(shape((rows, width), BF16) for _ in ks),
            2 * len(ks) * rows * cols * width,
            *args,
            scratch=(
                pltpu.VMEM((len(ks), rows, cols), BF16),
                pltpu.VMEM((len(ks), rows, width), BF16),
                pltpu.SemaphoreType.DMA((len(ks) * COPIES,)),
            ),
            smem=(0,),
            far_out=True,
        )

    made = dict(zip(range(half, count), project(tuple(range(half, count)))))
    made.update(zip(range(half), project(tuple(range(half)))))
    bit = 1
    while bit < count:
        for k in sorted((k for k in made if not k & bit), reverse=True):
            last = k == 0 and 2 * bit == count
            made[k] = call(
        add_kernel,
        shape((rows, width), BF16 if k or last else F32),
        rows * width,
        made[k],
        swap(made.pop(k ^ bit), "tp", bit),
            )
        bit *= 2
    mixer_out = made[0].astype(BF16)

    hidden = call(
        functools.partial(hidden_kernel, pieces, count),
        shape((slots_total, count * gate_parts[0].shape[1]), BF16),
        4 * count * slots_total * width * gate_parts[0].shape[1],
        *arrived,
        *gate_parts,
        *up_parts,
    )
    held = []
    for i, span in enumerate(spans):
        final = i == len(spans) - 1
        done = call(
            functools.partial(down_kernel, count),
            tuple(shape((slots_total // pieces, span), BF16) for _ in range(pieces)),
            2 * slots_total * span * count * down.shape[0],
            hidden,
            *down_parts[i],
        )
        held.append(
            call(
                functools.partial(combine_kernel, ep_size, room, len(held) if final else 0),
                shape((local_rows, width if final else span), BF16),
                6 * local_rows * slots_total * span,
                place,
                expert_ids,
                route_weight,
                *(held if final else []),
                *exchange_all(done),
                smem=(0,),
            )
        )
    expert_out = held[-1]
    return (mixer_out, expert_out)


def solution(mesh):
    placed = (
        P(("ep", "tp"), None),
        P(),
        P(None, "tp"),
        P(None, "tp"),
        P(None, "tp"),
        P("tp", None, None),
        P("tp", None, None),
        P("tp"),
        P("ep", "tp"),
        P("tp", None),
        P(("ep", "tp"), None),
        P(),
        P(("ep", "tp"), None),
        P(("ep", "tp"), None),
        P("ep", None, "tp"),
        P("ep", None, "tp"),
        P("ep", "tp", None),
    )
    return jax.shard_map(
        body,
        mesh=mesh,
        in_specs=placed,
        out_specs=(P(("ep", "tp"), None), P(("ep", "tp"), None)),
        check_vma=False,
    )
```

```python
import functools
import math

import jax
import jax.numpy as jnp
from jax import lax
from jax.experimental import pallas as pl
from jax.experimental.pallas import tpu as pltpu
from jax.sharding import PartitionSpec as P


epsilon = 1e-06
gate_const = 8.0
SUB = 8
EP, TP = "ep", "tp"
SPARE = 6
SPLIT = 7
F32 = jnp.float32
BF16 = jnp.bfloat16


def dotf(a, b):
    return jnp.dot(a, b, preferred_element_type=F32)


def swap(block, axis, bit):
    size = lax.axis_size(axis)
    return lax.ppermute(block, axis, [(i, i ^ bit) for i in range(size)])


def from_behind(block, axes):
    size = math.prod(lax.axis_size(a) for a in axes)
    return lax.ppermute(block, axes, [(i, i + 1) for i in range(size - 1)])


def exchange(block, axis):
    return lax.all_to_all(block, axis, split_axis=0, concat_axis=0, tiled=True)


def tp_bits():
    size, bits = lax.axis_size(TP), []
    while size > 1:
        size //= 2
        bits.append(size)
    return bits


def spread(block):
    held = {0: block}
    for bit in tp_bits():
        held.update({k ^ bit: swap(v, TP, bit) for k, v in list(held.items())})
    return [held[k] for k in range(len(held))]


def cost(flops, moved, transcendentals=0):
    return pl.CostEstimate(flops=flops, bytes_accessed=moved, transcendentals=transcendentals)


def call(
    kernel, outs, flops, *args, scratch=(), smem=(), grid=None, maps=(), out_maps=None, far=(), alone=False,
    stay=False, far_out=False
):
    sizes = [a.size * a.dtype.itemsize for a in args]
    sizes += [o.size * o.dtype.itemsize for o in jax.tree.leaves(outs)]
    moved = sum(sizes)
    if not alone:
        held = moved + sum(math.prod(v.shape) * v.dtype.itemsize for v in scratch if hasattr(v.dtype, "itemsize"))

    def spec(i, a):
        if i in smem:
            return pl.BlockSpec(memory_space=pltpu.SMEM)
        if i in far:
            return pl.BlockSpec(memory_space=pl.ANY)
        if grid is None:
            return pl.BlockSpec(memory_space=pltpu.VMEM)
        if i in maps:
            return pl.BlockSpec(*maps[i])
        return pl.BlockSpec(a.shape, lambda n, rank=a.ndim: (0,) * rank)

    return pl.pallas_call(
        kernel,
        out_shape=jax.tree.map(lambda o: pltpu.VMEM(o.shape, o.dtype), outs) if stay else outs,
        grid=() if grid is None else (grid,),
        in_specs=[spec(i, a) for i, a in enumerate(args)],
        out_specs=jax.tree.map(
            lambda o: pl.BlockSpec(*out_maps)
            if grid
            else pl.BlockSpec(memory_space=pl.ANY if far_out else pltpu.VMEM),
            outs,
        ),
        scratch_shapes=list(scratch),
        cost_estimate=cost(flops, moved),
        compiler_params=pltpu.CompilerParams(
            vmem_limit_bytes=None if grid or alone else held + (SPARE << 20)
        ),
    )(*args)


def normed_rows(x_ref, gain_ref):
    values = x_ref[...].astype(F32)
    inv = lax.rsqrt(jnp.mean(values * values, axis=-1, keepdims=True) + epsilon)
    return (values * inv * gain_ref[...][None, :].astype(F32)).astype(BF16)


def norm_kernel(x_ref, gain_ref, out_ref):
    normed = normed_rows(x_ref, gain_ref)
    out_ref[...] = dotf(time_order(x_ref.shape[0]), normed).astype(BF16)


def time_order(rows, back=False):
    steps = rows // SUB
    r = lax.broadcasted_iota(jnp.int32, (rows, rows), 1 if back else 0)
    t = lax.broadcasted_iota(jnp.int32, (rows, rows), 0 if back else 1)
    return (t == (r % SUB) * steps + r // SUB).astype(F32).astype(BF16)


def stage_kernel(n, *refs):
    copies = [pltpu.make_async_copy(refs[i], refs[n + i], refs[2 * n].at[i]) for i in range(n)]
    for copy in copies:
        copy.start()
    for copy in copies:
        copy.wait()


def stack_kernel(*refs):
    *parts, out_ref, sems = refs
    rows = parts[0].shape[0]
    copies = [
        pltpu.make_async_copy(p, out_ref.at[i * rows : (i + 1) * rows, :], sems.at[i])
        for i, p in enumerate(parts)
    ]
    for copy in copies:
        copy.start()
    for copy in copies:
        copy.wait()


def prepare_kernel(spans, down_ref, recur_ref, inject_ref, gates_ref, *outs):
    at = 0
    for out, span in zip(outs, spans):
        out[...] = down_ref[:, at : at + span]
        at += span
    gates_kernel(recur_ref, inject_ref, gates_ref)


def split3(values):
    high = values.astype(BF16)
    rest = values - high.astype(F32)
    middle = rest.astype(BF16)
    return high, middle, (rest - middle.astype(F32)).astype(BF16)


def gates_kernel(recur_ref, inject_ref, out_ref):
    groups, width, _ = out_ref.shape
    head = recur_ref.shape[1]
    j = lax.broadcasted_iota(jnp.int32, (head, width), 0)
    c = lax.broadcasted_iota(jnp.int32, (head, width), 1)
    repeat = (c % head == j).astype(F32).astype(BF16)
    r = lax.broadcasted_iota(jnp.int32, (width, width), 0)
    c = lax.broadcasted_iota(jnp.int32, (width, width), 1)
    same = r // head == c // head
    for g in range(groups):
        for i, ref in enumerate((recur_ref, inject_ref)):
            wide = dotf(ref[g * width : (g + 1) * width, :], repeat)
            out_ref[g, :, i * width : (i + 1) * width] = jnp.where(same, wide, 0.0).astype(BF16)


def kick_kernel(kick_ref, out_ref):
    count, rows, cols = out_ref.shape
    heads = kick_ref.shape[0]
    h = lax.broadcasted_iota(jnp.int32, (heads, cols), 0)
    c = lax.broadcasted_iota(jnp.int32, (heads, cols), 1)
    widen = (c // (cols // heads) == h).astype(F32).astype(BF16)
    order = time_order(rows)
    for b in range(count):
        parts = split3(jnp.transpose(kick_ref[:, b * rows : (b + 1) * rows]))
        high, middle, small = [dotf(dotf(order, part).astype(BF16), widen) for part in parts]
        out_ref[b] = high + (middle + small)


def lead_kernel(gain_ref, wb_ref, *refs):
    out_ref = refs[-1]
    rows = jnp.concatenate([normed_rows(r, gain_ref) for r in refs[:-1]], axis=0)
    made = dotf(rows, wb_ref[...]).astype(BF16).astype(F32)
    for i in range(out_ref.shape[0]):
        out_ref[i] = made[i * out_ref.shape[1] : (i + 1) * out_ref.shape[1]]


def block_kernel(taps_count, count, ks, held, place_ref, *refs):
    edges, refs = refs[:held], refs[held:]
    n = len(ks)
    kick_ref, wb_ref, wg_ref, taps_ref, gates_ref, slow_ref, lead_ref = refs[:7]
    xs, refs = refs[7 : 7 + n], refs[7 + n :]
    body_ref, edge_ref = refs[:2]
    scratch = refs[len(refs) - 3 :]
    me = place_ref[0]
    for i, k in enumerate(ks):
        one_block(
            taps_count,
            xs[i],
            lead_ref[i],
            kick_ref.at[me ^ k],
            wb_ref,
            wg_ref,
            taps_ref,
            gates_ref,
            slow_ref,
            body_ref.at[i],
            edge_ref.at[i],
            *scratch,
        )
    if held:
        decay = jnp.ones((1, edge_ref.shape[2]), F32)
        state = jnp.zeros((1, edge_ref.shape[2]), F32)
        tots = ends_of((*edges, edge_ref))
        for b in range(count):
            decay, state = chain(decay, state, choose(tots, me ^ b))
        total_ref = refs[2]
        total_ref[0:1, :] = decay
        total_ref[1:2, :] = state


def one_block(
    taps_count,
    x_ref,
    bt,
    kick_ref,
    wb_ref,
    wg_ref,
    taps_ref,
    gates_ref,
    slow_ref,
    body_ref,
    edge_ref,
    xf_ref,
    bg_ref,
    pre_ref,
):
    _, rows, cols = body_ref.shape
    steps = rows // SUB
    lead = taps_count - 1
    x = x_ref[...]
    bt = bt[bt.shape[0] - lead :]
    xf_ref[lead * SUB :, :] = dotf(x, wb_ref[...]).astype(BF16).astype(F32)
    sub = lax.broadcasted_iota(jnp.int32, (SUB, cols), 0)
    for m in range(lead):
        at = rows + m * SUB
        shifted = pltpu.roll(xf_ref[at : at + SUB, :], 1, 0)
        xf_ref[m * SUB : (m + 1) * SUB, :] = jnp.where(sub == 0, bt[m : m + 1], shifted)
    taps = taps_ref[...].astype(F32)
    conv = taps[0:1] * xf_ref[:rows, :]
    for k in range(1, taps_count):
        conv = conv + taps[k : k + 1] * xf_ref[k * SUB : k * SUB + rows, :]
    xf_ref[:rows, :] = conv
    low = conv.astype(BF16)
    width = gates_ref.shape[1]
    for g in range(cols // width):
        pre = dotf(low[:, g * width : (g + 1) * width], gates_ref[g])
        pre_ref[:, g * width : (g + 1) * width] = pre[:, :width]
        pre_ref[:, cols + g * width : cols + (g + 1) * width] = pre[:, width:]
    bg_ref[...] = dotf(x, wg_ref[...]).astype(BF16).astype(F32)
    slow = slow_ref[...] * (-gate_const)

    def step(j, carry):
        state, decay = carry
        at = pl.ds(pl.multiple_of(j * SUB, SUB), SUB)
        recur = jax.nn.sigmoid(pre_ref[at, :cols])
        inject = jax.nn.sigmoid(pre_ref[at, cols:])
        log_decay = recur * slow + kick_ref[at, :]
        a = jnp.exp(log_decay)
        u = 2.0 * log_decay
        series = 1.0 / 40320.0
        for c in (5040.0, 720.0, 120.0, 24.0, 6.0, 2.0, 1.0):
            series = series * u + 1.0 / c
        gone = jnp.where(u > -0.5, -u * series, 1.0 - a * a)
        drive = jnp.sqrt(gone) * inject * xf_ref[at, :]
        state = a * state + drive
        decay = a * decay
        opening = jax.nn.gelu(bg_ref[at, :])
        return state, decay, state * opening, decay * opening

    unroll = 4 if steps % 4 == 0 else 2

    def several(i, carry):
        at = pl.ds(pl.multiple_of(i * unroll * SUB, unroll * SUB), unroll * SUB)
        locs, accs = [], []
        for n in range(unroll):
            *carry, loc, acc = step(i * unroll + n, carry)
            locs.append(loc)
            accs.append(acc)
        body_ref[0, at, :] = jnp.concatenate(locs, axis=0).astype(BF16)
        body_ref[1, at, :] = jnp.concatenate(accs, axis=0).astype(BF16)
        return tuple(carry)

    state, decay = lax.fori_loop(
        0,
        steps // unroll,
        several,
        (jnp.zeros((SUB, cols), F32), jnp.ones((SUB, cols), F32)),
    )
    for d in (1, 2, 4):
        behind_state = pltpu.roll(state, d, 0)
        behind_decay = pltpu.roll(decay, d, 0)
        state = jnp.where(sub >= d, decay * behind_state + state, state)
        decay = jnp.where(sub >= d, decay * behind_decay, decay)
    edge_ref[:SUB, :] = jnp.where(sub == 0, 0.0, pltpu.roll(state, 1, 0))
    edge_ref[SUB : 2 * SUB, :] = jnp.where(sub == 0, 1.0, pltpu.roll(decay, 1, 0))
    edge_ref[2 * SUB :, :] = jnp.where(
        sub == 0,
        jnp.broadcast_to(decay[SUB - 1 :], sub.shape),
        jnp.broadcast_to(state[SUB - 1 :], sub.shape),
    )


def chain(decay, state, part):
    return part[0:1] * decay, part[0:1] * state + part[1:2]


def choose(parts, index):
    picked = parts[0]
    for k in range(1, len(parts)):
        picked = jnp.where(index == k, parts[k], picked)
    return picked


def ends_of(edge_refs):
    return [
        r[i, 2 * SUB : 2 * SUB + 2] for r in edge_refs for i in range(r.shape[0])
    ]


def pack_kernel(places, *refs):
    for i, (a, n) in enumerate(places):
        refs[-1][i] = refs[a][n] if len(refs[a].shape) == 3 else refs[a][...]


def entering(total):
    size = lax.axis_size(EP)
    bits = [1 << b for b in range(size.bit_length() - 1)]
    arrays, holds = [total], [[0]]
    for stage in (bits[:2], *([b] for b in bits[2:])):
        masks = [0]
        for bit in stage:
            masks += [m ^ bit for m in masks]
        known = [m for hold in holds for m in hold]
        packed = total
        if len(known) > 1:
            places = [(a, n) for a, hold in enumerate(holds) for n in range(len(hold))]
            packed = call(
                functools.partial(pack_kernel, places),
                jax.ShapeDtypeStruct((len(known), *total.shape), F32),
                1000,
                *arrays,
            )
            arrays, holds = [packed], [known]
        for m in masks[:0:-1]:
            arrays.append(swap(packed, EP, m))
            holds.append([k ^ m for k in known])
    return arrays, holds


def mix_kernel(holds, arrays, ks, place_ref, *refs):
    totals, refs = refs[: len(holds)], refs[len(holds) :]
    edges, refs = refs[:arrays], refs[arrays:]
    given, outs, all_ref = refs[: -len(ks) - 1], refs[-len(ks) - 1 : -1], refs[-1]
    for ref, hold in zip(totals, holds):
        for n, m in enumerate(hold):
            all_ref[m] = ref[n] if len(ref.shape) == 3 else ref[...]
    me, here = place_ref[0], place_ref[1]

    def pass_on(b, state):
        part = all_ref[here ^ b]
        return part[0:1] * state + part[1:2]

    rows, cols = outs[0].shape
    entry = lax.fori_loop(0, here, pass_on, jnp.zeros((1, cols), F32))
    tots = ends_of(edges)
    prefs = [r[i, : 2 * SUB] for r in edges for i in range(r.shape[0])]
    bodies = [r.at[i] for r in given for i in range(r.shape[0])]
    entries = []
    decay = jnp.ones((1, cols), F32)
    for b in range(len(tots)):
        entries.append(entry)
        decay, entry = chain(decay, entry, choose(tots, me ^ b))
    order = time_order(rows, back=True)
    for n, k in enumerate(ks):
        carried = choose(entries, me ^ k)
        lift = prefs[k][:SUB] + prefs[k][SUB:] * carried
        lift = jnp.broadcast_to(lift[None], (rows // SUB, SUB, cols)).reshape(rows, cols)
        mixed = (bodies[n][0].astype(F32) + bodies[n][1].astype(F32) * lift).astype(BF16)
        outs[n][...] = dotf(order, mixed).astype(BF16)


def out_kernel(*refs):
    out_ref, n = refs[-1], len(refs) // 2
    total = dotf(refs[0][...], refs[n][...])
    for i in range(1, n):
        total = total + dotf(refs[i][...], refs[n + i][...])
    out_ref[...] = total.astype(out_ref.dtype)


def add_kernel(a_ref, b_ref, out_ref):
    out_ref[...] = (a_ref[...].astype(F32) + b_ref[...].astype(F32)).astype(out_ref.dtype)


def slots_of(ids, flip, room, experts, axis):
    tokens = ids.shape[1 - axis]
    picks = ids.shape[axis]
    shape = (experts, tokens) if axis == 0 else (tokens, experts)
    number = lax.broadcasted_iota(jnp.int32, shape, axis)
    cut = [ids[k : k + 1, :] if axis == 0 else ids[:, k : k + 1] for k in range(picks)]
    hot = [(c == number).astype(F32) for c in cut]
    r = lax.broadcasted_iota(jnp.int32, (tokens, tokens), 0)
    c = lax.broadcasted_iota(jnp.int32, (tokens, tokens), 1)
    every = functools.reduce(lambda a, b: a + b, hot).astype(BF16)
    if axis == 0:
        seen = dotf(every, (r < c).astype(F32).astype(BF16))
    else:
        seen = dotf((c < r).astype(F32).astype(BF16), every)
    return [
        (c ^ flip) * room + jnp.sum(h * seen, axis=axis, keepdims=True).astype(jnp.int32)
        for c, h in zip(cut, hot)
    ]


def dispatch_kernel(experts, room, place_ref, x_ref, gain_ref, ids_ref, *outs):
    values = x_ref[...].astype(F32)
    inv = lax.rsqrt(jnp.mean(values * values, axis=-1, keepdims=True) + epsilon)
    normed = (values * inv * gain_ref[...][None, :].astype(F32)).astype(BF16)
    slots = slots_of(ids_ref[...], place_ref[2], room, experts, 0)
    number = lax.broadcasted_iota(jnp.int32, (experts * room, values.shape[0]), 0)
    table = functools.reduce(jnp.logical_or, [number == s for s in slots])
    rows = dotf(table.astype(F32).astype(BF16), normed).astype(BF16)
    at = 0
    for out in outs:
        out[...] = rows[at : at + out.shape[0]]
        at += out.shape[0]


def table_kernel(experts, room, place_ref, ids_ref, weight_ref, out_ref):
    slots = slots_of(ids_ref[...], place_ref[2], room, experts, 1)
    number = lax.broadcasted_iota(jnp.int32, out_ref.shape[1:], 1)
    table = jnp.zeros(number.shape, F32)
    for k, s in enumerate(slots):
        table = jnp.where(number == s, weight_ref[:, k : k + 1], table)
    for i, part in enumerate(split3(table)):
        out_ref[i] = part


def combine_kernel(held, table_ref, *refs):
    parts, out_ref = refs[held:-1], refs[-1]
    value = stacked(parts)
    high, middle, small = [dotf(table_ref[i], value) for i in range(3)]
    at = 0
    for ref in refs[:held]:
        out_ref[:, at : at + ref.shape[1]] = ref[...]
        at += ref.shape[1]
    out_ref[:, at:] = (high + (middle + small)).astype(BF16)


def exchange_all(pieces):
    if len(pieces) == 1:
        return [exchange(pieces[0], EP)]
    got = {0: pieces[0]}
    for m in range(1, len(pieces)):
        got[m] = swap(pieces[m], EP, m)
    return [got[m] for m in range(len(pieces))]


def stacked(refs):
    values = [r[...] for r in refs]
    return values[0] if len(values) == 1 else jnp.concatenate(values, axis=0)


def stage_pairs_kernel(n, *refs):
    outs, sems = refs[2 * n : 3 * n], refs[3 * n]
    copies = []
    for i, out in enumerate(outs):
        span = out.shape[1] // 2
        for part in range(2):
            copies.append(
                pltpu.make_async_copy(
                    refs[part * n + i],
                    out.at[:, part * span : (part + 1) * span],
                    sems.at[2 * i + part],
                )
            )
            copies[-1].start()
    for copy in copies:
        copy.wait()


def hidden_kernel(pieces, *refs):
    arrived, (*wides, out_ref, x_ref, sems) = refs[:pieces], refs[pieces:]
    rows, span = arrived[0].shape[0], wides[0].shape[1] // 2
    loads = [
        pltpu.make_async_copy(a, x_ref.at[i * rows : (i + 1) * rows, :], sems.at[i])
        for i, a in enumerate(arrived)
    ]
    for load in loads:
        load.start()
    for load in loads:
        load.wait()
    x = x_ref[...]
    for i, wide in enumerate(wides):
        both = dotf(x, wide[...])
        done = jax.nn.silu(both[:, :span]) * both[:, span:]
        out_ref[:, i * span : (i + 1) * span] = done.astype(BF16)


def down_kernel(early, n, h_ref, *refs):
    parts, outs, (down_ref, sems) = refs[:n], refs[n:-2], refs[-2:]
    rows = parts[-1].shape[0]
    loads = [
        pltpu.make_async_copy(p, down_ref.at[i * rows : (i + 1) * rows, :], sems.at[i])
        for i, p in enumerate(parts[early:])
    ]
    for load in loads:
        load.start()
    at = 0
    total = None
    for part in parts[:early]:
        done = dotf(h_ref[:, at : at + part.shape[0]], part[...])
        total = done if total is None else total + done
        at += part.shape[0]
    for load in loads:
        load.wait()
    done = dotf(h_ref[:, at:], down_ref[...])
    total = done if total is None else total + done
    at = 0
    for out in outs:
        out[...] = total[at : at + out.shape[0]].astype(BF16)
        at += out.shape[0]


def body(
    mix_tokens,
    mix_gain,
    w_branch,
    w_gate_branch,
    conv_taps,
    recur_gate_w,
    inject_gate_w,
    decay_logit,
    decay_kick,
    w_mix_out,
    moe_tokens,
    moe_gain,
    expert_ids,
    route_weight,
    expert_gate_w,
    expert_up_w,
    expert_down_w,
):
    shape = jax.ShapeDtypeStruct
    me = lax.axis_index(TP)
    here = lax.axis_index(EP)
    count = lax.axis_size(TP)
    ep_size = lax.axis_size(EP)
    direct = 1 < ep_size <= 8
    place = jnp.stack([me, here, here if direct else 0 * here]).astype(jnp.int32)
    rows, width = mix_tokens.shape
    cols = w_branch.shape[1]
    taps_count = conv_taps.shape[0]
    half = max(count // 2, 1)

    lead = from_behind(mix_tokens[rows - SUB :], (EP, TP))

    local_rows, top_count = expert_ids.shape
    slots_total = 2 * local_rows * top_count
    room = slots_total // ep_size
    pieces = ep_size if direct else 1
    outgoing = call(
        functools.partial(dispatch_kernel, ep_size, room),
        tuple(shape((slots_total // pieces, width), BF16) for _ in range(pieces)),
        2 * local_rows * slots_total * width,
        place,
        moe_tokens,
        moe_gain,
        expert_ids.T,
        smem=(0,),
        alone=True,
    )
    arrived = exchange_all(outgoing)
    gate_parts = spread(expert_gate_w[0])
    up_parts = spread(expert_up_w[0])
    down = expert_down_w[0]
    first = width * SPLIT // 16 // 128 * 128
    spans = (first, width - first)
    head_count, head_dim, _ = recur_gate_w.shape
    group = 256 if cols % 256 == 0 and 256 % head_dim == 0 else cols
    gates, *down_cut = call(
        functools.partial(prepare_kernel, spans),
        (
            shape((cols // group, group, 2 * group), BF16),
            *[shape((down.shape[0], span), BF16) for span in spans],
        ),
        4 * cols * group * head_dim,
        down,
        recur_gate_w.reshape(cols, head_dim),
        inject_gate_w.reshape(cols, head_dim),
    )
    down_parts = [spread(part) for part in down_cut]

    mixer_in = call(
        norm_kernel,
        shape((rows, width), BF16),
        2 * rows * rows * width,
        mix_tokens,
        mix_gain,
        alone=True,
    )
    leads = spread(lead)
    blocks = spread(mixer_in)

    slowness = jax.nn.softplus(-decay_logit)[None, :]
    kick = call(
        kick_kernel,
        shape((count, rows, cols), F32),
        6 * count * rows * rows * head_count,
        decay_kick.T,
        stay=True,
    )
    parts = {}

    def run_blocks(ks):
        heads = call(
            lead_kernel,
            shape((len(ks), leads[0].shape[0], cols), F32),
            2 * len(ks) * leads[0].shape[0] * width * cols,
            mix_gain,
            w_branch,
            *[leads[k] for k in ks],
            stay=True,
        )
        outs = (
            shape((len(ks), 2, rows, cols), BF16),
            shape((len(ks), 3 * SUB, cols), F32),
        )
        edges = []
        if ks[-1] == count - 1:
            outs += (shape((2, cols), F32),)
            edges = [parts[g][1] for g in sorted(parts)]
        made = call(
            functools.partial(block_kernel, taps_count, count, ks, len(edges)),
            outs,
            2 * len(ks) * rows * cols * (2 * width + 2 * group),
            place,
            *edges,
            kick,
            w_branch,
            w_gate_branch,
            conv_taps,
            gates,
            slowness,
            heads,
            *[blocks[k] for k in ks],
            scratch=(
                pltpu.VMEM((rows + (taps_count - 1) * SUB, cols), F32),
                pltpu.VMEM((rows, cols), F32),
                pltpu.VMEM((rows, 2 * cols), F32),
            ),
            smem=(0,),
            stay=True,
        )
        parts[ks] = made

    run_blocks(tuple(range(half)))
    for k in range(half, count):
        run_blocks((k,))
    groups = sorted(parts)
    edges = [parts[ks][1] for ks in groups]
    totals, holds = entering(parts[groups[-1]][2])

    near_down = call(
        stack_kernel,
        shape((half * down.shape[0], spans[-1]), BF16),
        1000,
        *down_parts[-1][:half],
        scratch=(pltpu.SemaphoreType.DMA((half,)),),
        far=tuple(range(half)),
        stay=True,
    )
    pair = min(count, 2)
    wides = [w_mix_out] + [swap(w_mix_out, TP, 1)] * (pair - 1)
    wides = call(
        functools.partial(stage_kernel, pair),
        tuple(shape(w.shape, BF16) for w in wides),
        1000,
        *wides,
        scratch=(pltpu.SemaphoreType.DMA((pair,)),),
        far=tuple(range(pair)),
        stay=True,
    )
    mixed = {}
    for g in [tuple(range(half, count)), tuple(range(half))]:
        if g:
            args = [place, *totals, *edges, *[parts[p][0] for p in groups if set(p) <= set(g)]]
            made = call(
                functools.partial(mix_kernel, holds, len(groups), g),
                tuple(shape((rows, cols), BF16) for _ in g),
                2 * len(g) * rows * rows * cols,
                *args,
                scratch=(pltpu.VMEM((ep_size, 2, cols), F32),),
                smem=(0,),
                stay=True,
            )
            mixed.update(zip(g, made))
    made = {}
    for k in range(count - pair, -1, -pair):
        mine = [mixed[k]] + [swap(mixed[k + i], TP, 1) for i in range(1, pair)]
        made[k] = call(
            out_kernel,
            shape((rows, width), BF16 if k or count <= 2 else F32),
            2 * pair * rows * cols * width,
            *mine,
            *wides,
            stay=k == 0 and count > 2,
        )
    bit = pair
    while bit < count:
        for k in sorted((k for k in made if not k & bit), reverse=True):
            last = k == 0 and 2 * bit == count
            made[k] = call(
                add_kernel,
                shape((rows, width), BF16 if k or last else F32),
                rows * width,
                made[k],
                swap(made.pop(k ^ bit), TP, bit),
            )
        bit *= 2
    mixer_out = made[0]

    inner, span = gate_parts[0].shape
    staged = call(
        functools.partial(stage_pairs_kernel, count),
        tuple(shape((inner, 2 * span), BF16) for _ in range(count)),
        1000,
        *gate_parts,
        *up_parts,
        scratch=(pltpu.SemaphoreType.DMA((2 * count,)),),
        far=tuple(range(2 * count)),
        stay=True,
    )
    hidden = call(
        functools.partial(hidden_kernel, pieces),
        shape((slots_total, count * span), BF16),
        4 * count * slots_total * width * span,
        *arrived,
        *staged,
        scratch=(pltpu.VMEM((slots_total, width), BF16), pltpu.SemaphoreType.DMA((pieces,))),
        far=tuple(range(pieces)),
        stay=True,
    )
    table = call(
        functools.partial(table_kernel, ep_size, room),
        shape((3, local_rows, slots_total), BF16),
        1000,
        place,
        expert_ids,
        route_weight,
        smem=(0,),
        stay=True,
    )
    held = []
    for i, span in enumerate(spans):
        final = i == len(spans) - 1
        near = [near_down] if final else []
        far = down_parts[i][half:] if final else down_parts[i]
        done = call(
            functools.partial(down_kernel, len(near), len(near) + len(far)),
            tuple(shape((slots_total // pieces, span), BF16) for _ in range(pieces)),
            2 * slots_total * span * count * down.shape[0],
            hidden,
            *near,
            *far,
            scratch=(
                pltpu.VMEM((len(far) * down.shape[0], span), BF16),
                pltpu.SemaphoreType.DMA((len(far),)),
            ),
            far=tuple(range(1 + len(near), 1 + len(near) + len(far))),
        )
        held.append(
            call(
                functools.partial(combine_kernel, len(held) if final else 0),
                shape((local_rows, width if final else span), BF16),
                6 * local_rows * slots_total * span,
                table,
                *(held if final else []),
                *exchange_all(done),
                stay=not final,
            )
        )
    expert_out = held[-1]
    return (mixer_out, expert_out)


def solution(mesh):
    placed = (
        P((EP, TP), None),
        P(),
        P(None, TP),
        P(None, TP),
        P(None, TP),
        P(TP, None, None),
        P(TP, None, None),
        P(TP),
        P(EP, TP),
        P(TP, None),
        P((EP, TP), None),
        P(),
        P((EP, TP), None),
        P((EP, TP), None),
        P(EP, None, TP),
        P(EP, None, TP),
        P(EP, TP, None),
    )
    return jax.shard_map(
        body,
        mesh=mesh,
        in_specs=placed,
        out_specs=(P((EP, TP), None), P((EP, TP), None)),
        check_vma=False,
    )
```

```python
import functools
import math

import jax
import jax.numpy as jnp
from jax import lax
from jax.experimental import pallas as pl
from jax.experimental.pallas import tpu as pltpu
from jax.sharding import PartitionSpec as P


epsilon = 1e-06
gate_const = 8.0
SUB = 8
EP, TP = "ep", "tp"
SPARE = 6
SPLIT = 7
F32 = jnp.float32
BF16 = jnp.bfloat16


def dotf(a, b):
    return jnp.dot(a, b, preferred_element_type=F32)


def swap(block, axis, bit):
    size = lax.axis_size(axis)
    return lax.ppermute(block, axis, [(i, i ^ bit) for i in range(size)])


def from_behind(block, axes):
    size = math.prod(lax.axis_size(a) for a in axes)
    return lax.ppermute(block, axes, [(i, i + 1) for i in range(size - 1)])


def exchange(block, axis):
    return lax.all_to_all(block, axis, split_axis=0, concat_axis=0, tiled=True)


def tp_bits():
    size, bits = lax.axis_size(TP), []
    while size > 1:
        size //= 2
        bits.append(size)
    return bits


def spread(block):
    held = {0: block}
    for bit in tp_bits():
        held.update({k ^ bit: swap(v, TP, bit) for k, v in list(held.items())})
    return [held[k] for k in range(len(held))]


def cost(flops, moved, transcendentals=0):
    return pl.CostEstimate(flops=flops, bytes_accessed=moved, transcendentals=transcendentals)


def call(
    kernel, outs, flops, *args, scratch=(), smem=(), grid=None, maps=(), out_maps=None, far=(), alone=False,
    stay=False, far_out=False
):
    sizes = [a.size * a.dtype.itemsize for a in args]
    sizes += [o.size * o.dtype.itemsize for o in jax.tree.leaves(outs)]
    moved = sum(sizes)
    if not alone:
        held = moved + sum(math.prod(v.shape) * v.dtype.itemsize for v in scratch if hasattr(v.dtype, "itemsize"))

    def spec(i, a):
        if i in smem:
            return pl.BlockSpec(memory_space=pltpu.SMEM)
        if i in far:
            return pl.BlockSpec(memory_space=pl.ANY)
        if grid is None:
            return pl.BlockSpec(memory_space=pltpu.VMEM)
        if i in maps:
            return pl.BlockSpec(*maps[i])
        return pl.BlockSpec(a.shape, lambda n, rank=a.ndim: (0,) * rank)

    return pl.pallas_call(
        kernel,
        out_shape=jax.tree.map(lambda o: pltpu.VMEM(o.shape, o.dtype), outs) if stay else outs,
        grid=() if grid is None else (grid,),
        in_specs=[spec(i, a) for i, a in enumerate(args)],
        out_specs=jax.tree.map(
            lambda o: pl.BlockSpec(*out_maps)
            if grid
            else pl.BlockSpec(memory_space=pl.ANY if far_out else pltpu.VMEM),
            outs,
        ),
        scratch_shapes=list(scratch),
        cost_estimate=cost(flops, moved),
        compiler_params=pltpu.CompilerParams(
            vmem_limit_bytes=None if grid or alone else held + (SPARE << 20)
        ),
    )(*args)


def normed_rows(x_ref, gain_ref):
    values = x_ref[...].astype(F32)
    inv = lax.rsqrt(jnp.mean(values * values, axis=-1, keepdims=True) + epsilon)
    return (values * inv * gain_ref[...][None, :].astype(F32)).astype(BF16)


def norm_kernel(x_ref, gain_ref, out_ref):
    normed = normed_rows(x_ref, gain_ref)
    out_ref[...] = dotf(time_order(x_ref.shape[0]), normed).astype(BF16)


def time_order(rows, back=False):
    steps = rows // SUB
    r = lax.broadcasted_iota(jnp.int32, (rows, rows), 1 if back else 0)
    t = lax.broadcasted_iota(jnp.int32, (rows, rows), 0 if back else 1)
    return (t == (r % SUB) * steps + r // SUB).astype(F32).astype(BF16)


def stage_kernel(n, *refs):
    copies = [pltpu.make_async_copy(refs[i], refs[n + i], refs[2 * n].at[i]) for i in range(n)]
    for copy in copies:
        copy.start()
    for copy in copies:
        copy.wait()


def stack_kernel(*refs):
    *parts, out_ref, sems = refs
    rows = parts[0].shape[0]
    copies = [
        pltpu.make_async_copy(p, out_ref.at[i * rows : (i + 1) * rows, :], sems.at[i])
        for i, p in enumerate(parts)
    ]
    for copy in copies:
        copy.start()
    for copy in copies:
        copy.wait()


def prepare_kernel(spans, down_ref, recur_ref, inject_ref, gates_ref, *outs):
    at = 0
    for out, span in zip(outs, spans):
        out[...] = down_ref[:, at : at + span]
        at += span
    gates_kernel(recur_ref, inject_ref, gates_ref)


def split3(values):
    high = values.astype(BF16)
    rest = values - high.astype(F32)
    middle = rest.astype(BF16)
    return high, middle, (rest - middle.astype(F32)).astype(BF16)


def gates_kernel(recur_ref, inject_ref, out_ref):
    groups, width, _ = out_ref.shape
    head = recur_ref.shape[1]
    j = lax.broadcasted_iota(jnp.int32, (head, width), 0)
    c = lax.broadcasted_iota(jnp.int32, (head, width), 1)
    repeat = (c % head == j).astype(F32).astype(BF16)
    r = lax.broadcasted_iota(jnp.int32, (width, width), 0)
    c = lax.broadcasted_iota(jnp.int32, (width, width), 1)
    same = r // head == c // head
    for g in range(groups):
        for i, ref in enumerate((recur_ref, inject_ref)):
            wide = dotf(ref[g * width : (g + 1) * width, :], repeat)
            out_ref[g, :, i * width : (i + 1) * width] = jnp.where(same, wide, 0.0).astype(BF16)


def kick_kernel(kick_ref, out_ref):
    count, rows, cols = out_ref.shape
    heads = kick_ref.shape[0]
    h = lax.broadcasted_iota(jnp.int32, (heads, cols), 0)
    c = lax.broadcasted_iota(jnp.int32, (heads, cols), 1)
    widen = (c // (cols // heads) == h).astype(F32).astype(BF16)
    order = time_order(rows)
    for b in range(count):
        parts = split3(jnp.transpose(kick_ref[:, b * rows : (b + 1) * rows]))
        high, middle, small = [dotf(dotf(order, part).astype(BF16), widen) for part in parts]
        out_ref[b] = high + (middle + small)


def lead_kernel(gain_ref, wb_ref, *refs):
    out_ref = refs[-1]
    rows = jnp.concatenate([normed_rows(r, gain_ref) for r in refs[:-1]], axis=0)
    made = dotf(rows, wb_ref[...]).astype(BF16).astype(F32)
    for i in range(out_ref.shape[0]):
        out_ref[i] = made[i * out_ref.shape[1] : (i + 1) * out_ref.shape[1]]


def block_kernel(taps_count, count, ks, held, place_ref, *refs):
    edges, refs = refs[:held], refs[held:]
    n = len(ks)
    kick_ref, wb_ref, wg_ref, taps_ref, gates_ref, slow_ref, lead_ref = refs[:7]
    xs, refs = refs[7 : 7 + n], refs[7 + n :]
    body_ref, edge_ref = refs[:2]
    scratch = refs[len(refs) - 3 :]
    me = place_ref[0]
    for i, k in enumerate(ks):
        one_block(
            taps_count,
            xs[i],
            lead_ref[i],
            kick_ref.at[me ^ k],
            wb_ref,
            wg_ref,
            taps_ref,
            gates_ref,
            slow_ref,
            body_ref.at[i],
            edge_ref.at[i],
            *scratch,
        )
    if held:
        decay = jnp.ones((1, edge_ref.shape[2]), F32)
        state = jnp.zeros((1, edge_ref.shape[2]), F32)
        tots = ends_of((*edges, edge_ref))
        for b in range(count):
            decay, state = chain(decay, state, choose(tots, me ^ b))
        total_ref = refs[2]
        total_ref[0:1, :] = decay
        total_ref[1:2, :] = state


def one_block(
    taps_count,
    x_ref,
    bt,
    kick_ref,
    wb_ref,
    wg_ref,
    taps_ref,
    gates_ref,
    slow_ref,
    body_ref,
    edge_ref,
    xf_ref,
    bg_ref,
    pre_ref,
):
    _, rows, cols = body_ref.shape
    steps = rows // SUB
    lead = taps_count - 1
    x = x_ref[...]
    bt = bt[bt.shape[0] - lead :]
    xf_ref[lead * SUB :, :] = dotf(x, wb_ref[...]).astype(BF16).astype(F32)
    sub = lax.broadcasted_iota(jnp.int32, (SUB, cols), 0)
    for m in range(lead):
        at = rows + m * SUB
        shifted = pltpu.roll(xf_ref[at : at + SUB, :], 1, 0)
        xf_ref[m * SUB : (m + 1) * SUB, :] = jnp.where(sub == 0, bt[m : m + 1], shifted)
    taps = taps_ref[...].astype(F32)
    conv = taps[0:1] * xf_ref[:rows, :]
    for k in range(1, taps_count):
        conv = conv + taps[k : k + 1] * xf_ref[k * SUB : k * SUB + rows, :]
    xf_ref[:rows, :] = conv
    low = conv.astype(BF16)
    width = gates_ref.shape[1]
    for g in range(cols // width):
        pre = dotf(low[:, g * width : (g + 1) * width], gates_ref[g])
        pre_ref[:, g * width : (g + 1) * width] = pre[:, :width]
        pre_ref[:, cols + g * width : cols + (g + 1) * width] = pre[:, width:]
    bg_ref[...] = dotf(x, wg_ref[...]).astype(BF16).astype(F32)
    slow = slow_ref[...] * (-gate_const)

    def step(j, carry):
        state, decay = carry
        at = pl.ds(pl.multiple_of(j * SUB, SUB), SUB)
        recur = jax.nn.sigmoid(pre_ref[at, :cols])
        inject = jax.nn.sigmoid(pre_ref[at, cols:])
        log_decay = recur * slow + kick_ref[at, :]
        a = jnp.exp(log_decay)
        u = 2.0 * log_decay
        series = 1.0 / 720.0
        for c in (120.0, 24.0, 6.0, 2.0, 1.0):
            series = series * u + 1.0 / c
        gone = jnp.where(u > -0.2, -u * series, 1.0 - a * a)
        drive = jnp.sqrt(gone) * inject * xf_ref[at, :]
        state = a * state + drive
        decay = a * decay
        opening = jax.nn.gelu(bg_ref[at, :])
        return state, decay, state * opening, decay * opening

    unroll = 8 if steps % 8 == 0 else 2

    def several(i, carry):
        at = pl.ds(pl.multiple_of(i * unroll * SUB, unroll * SUB), unroll * SUB)
        locs, accs = [], []
        for n in range(unroll):
            *carry, loc, acc = step(i * unroll + n, carry)
            locs.append(loc)
            accs.append(acc)
        body_ref[0, at, :] = jnp.concatenate(locs, axis=0).astype(BF16)
        body_ref[1, at, :] = jnp.concatenate(accs, axis=0).astype(BF16)
        return tuple(carry)

    state, decay = lax.fori_loop(
        0,
        steps // unroll,
        several,
        (jnp.zeros((SUB, cols), F32), jnp.ones((SUB, cols), F32)),
    )
    for d in (1, 2, 4):
        behind_state = pltpu.roll(state, d, 0)
        behind_decay = pltpu.roll(decay, d, 0)
        state = jnp.where(sub >= d, decay * behind_state + state, state)
        decay = jnp.where(sub >= d, decay * behind_decay, decay)
    edge_ref[:SUB, :] = jnp.where(sub == 0, 0.0, pltpu.roll(state, 1, 0))
    edge_ref[SUB : 2 * SUB, :] = jnp.where(sub == 0, 1.0, pltpu.roll(decay, 1, 0))
    edge_ref[2 * SUB :, :] = jnp.where(
        sub == 0,
        jnp.broadcast_to(decay[SUB - 1 :], sub.shape),
        jnp.broadcast_to(state[SUB - 1 :], sub.shape),
    )


def chain(decay, state, part):
    return part[0:1] * decay, part[0:1] * state + part[1:2]


def choose(parts, index):
    picked = parts[0]
    for k in range(1, len(parts)):
        picked = jnp.where(index == k, parts[k], picked)
    return picked


def ends_of(edge_refs):
    return [
        r[i, 2 * SUB : 2 * SUB + 2] for r in edge_refs for i in range(r.shape[0])
    ]


def pack_kernel(places, *refs):
    for i, (a, n) in enumerate(places):
        refs[-1][i] = refs[a][n] if len(refs[a].shape) == 3 else refs[a][...]


def entering(total):
    size = lax.axis_size(EP)
    bits = [1 << b for b in range(size.bit_length() - 1)]
    arrays, holds = [total], [[0]]
    for stage in (bits[:2], *([b] for b in bits[2:])):
        masks = [0]
        for bit in stage:
            masks += [m ^ bit for m in masks]
        known = [m for hold in holds for m in hold]
        packed = total
        if len(known) > 1:
            places = [(a, n) for a, hold in enumerate(holds) for n in range(len(hold))]
            packed = call(
                functools.partial(pack_kernel, places),
                jax.ShapeDtypeStruct((len(known), *total.shape), F32),
                1000,
                *arrays,
            )
            arrays, holds = [packed], [known]
        for m in masks[:0:-1]:
            arrays.append(swap(packed, EP, m))
            holds.append([k ^ m for k in known])
    return arrays, holds


def mix_kernel(holds, arrays, ks, place_ref, *refs):
    totals, refs = refs[: len(holds)], refs[len(holds) :]
    edges, refs = refs[:arrays], refs[arrays:]
    given, outs, all_ref = refs[: -len(ks) - 1], refs[-len(ks) - 1 : -1], refs[-1]
    for ref, hold in zip(totals, holds):
        for n, m in enumerate(hold):
            all_ref[m] = ref[n] if len(ref.shape) == 3 else ref[...]
    me, here = place_ref[0], place_ref[1]

    def pass_on(b, state):
        part = all_ref[here ^ b]
        return part[0:1] * state + part[1:2]

    rows, cols = outs[0].shape
    entry = lax.fori_loop(0, here, pass_on, jnp.zeros((1, cols), F32))
    tots = ends_of(edges)
    prefs = [r[i, : 2 * SUB] for r in edges for i in range(r.shape[0])]
    bodies = [r.at[i] for r in given for i in range(r.shape[0])]
    entries = []
    decay = jnp.ones((1, cols), F32)
    for b in range(len(tots)):
        entries.append(entry)
        decay, entry = chain(decay, entry, choose(tots, me ^ b))
    order = time_order(rows, back=True)
    for n, k in enumerate(ks):
        carried = choose(entries, me ^ k)
        lift = prefs[k][:SUB] + prefs[k][SUB:] * carried
        lift = jnp.broadcast_to(lift[None], (rows // SUB, SUB, cols)).reshape(rows, cols)
        mixed = (bodies[n][0].astype(F32) + bodies[n][1].astype(F32) * lift).astype(BF16)
        outs[n][...] = dotf(order, mixed).astype(BF16)


def out_kernel(*refs):
    out_ref, n = refs[-1], len(refs) // 2
    total = dotf(refs[0][...], refs[n][...])
    for i in range(1, n):
        total = total + dotf(refs[i][...], refs[n + i][...])
    out_ref[...] = total.astype(out_ref.dtype)


def add_kernel(a_ref, b_ref, out_ref):
    out_ref[...] = (a_ref[...].astype(F32) + b_ref[...].astype(F32)).astype(out_ref.dtype)


def slots_of(ids, flip, room, experts, axis):
    tokens = ids.shape[1 - axis]
    picks = ids.shape[axis]
    shape = (experts, tokens) if axis == 0 else (tokens, experts)
    number = lax.broadcasted_iota(jnp.int32, shape, axis)
    cut = [ids[k : k + 1, :] if axis == 0 else ids[:, k : k + 1] for k in range(picks)]
    hot = [(c == number).astype(F32) for c in cut]
    r = lax.broadcasted_iota(jnp.int32, (tokens, tokens), 0)
    c = lax.broadcasted_iota(jnp.int32, (tokens, tokens), 1)
    every = functools.reduce(lambda a, b: a + b, hot).astype(BF16)
    if axis == 0:
        seen = dotf(every, (r < c).astype(F32).astype(BF16))
    else:
        seen = dotf((c < r).astype(F32).astype(BF16), every)
    return [
        (c ^ flip) * room + jnp.sum(h * seen, axis=axis, keepdims=True).astype(jnp.int32)
        for c, h in zip(cut, hot)
    ]


def dispatch_kernel(experts, room, place_ref, x_ref, gain_ref, ids_ref, *outs):
    values = x_ref[...].astype(F32)
    inv = lax.rsqrt(jnp.mean(values * values, axis=-1, keepdims=True) + epsilon)
    normed = (values * inv * gain_ref[...][None, :].astype(F32)).astype(BF16)
    slots = slots_of(ids_ref[...], place_ref[2], room, experts, 0)
    number = lax.broadcasted_iota(jnp.int32, (experts * room, values.shape[0]), 0)
    table = functools.reduce(jnp.logical_or, [number == s for s in slots])
    rows = dotf(table.astype(F32).astype(BF16), normed).astype(BF16)
    at = 0
    for out in outs:
        out[...] = rows[at : at + out.shape[0]]
        at += out.shape[0]


def table_kernel(experts, room, place_ref, ids_ref, weight_ref, out_ref):
    slots = slots_of(ids_ref[...], place_ref[2], room, experts, 1)
    number = lax.broadcasted_iota(jnp.int32, out_ref.shape[1:], 1)
    table = jnp.zeros(number.shape, F32)
    for k, s in enumerate(slots):
        table = jnp.where(number == s, weight_ref[:, k : k + 1], table)
    for i, part in enumerate(split3(table)):
        out_ref[i] = part


def combine_kernel(held, table_ref, *refs):
    parts, out_ref = refs[held:-1], refs[-1]
    value = stacked(parts)
    high, middle, small = [dotf(table_ref[i], value) for i in range(3)]
    at = 0
    for ref in refs[:held]:
        out_ref[:, at : at + ref.shape[1]] = ref[...]
        at += ref.shape[1]
    out_ref[:, at:] = (high + (middle + small)).astype(BF16)


def exchange_all(pieces):
    if len(pieces) == 1:
        return [exchange(pieces[0], EP)]
    got = {0: pieces[0]}
    for m in range(1, len(pieces)):
        got[m] = swap(pieces[m], EP, m)
    return [got[m] for m in range(len(pieces))]


def stacked(refs):
    values = [r[...] for r in refs]
    return values[0] if len(values) == 1 else jnp.concatenate(values, axis=0)


def stage_pairs_kernel(n, *refs):
    outs, sems = refs[2 * n : 3 * n], refs[3 * n]
    copies = []
    for i, out in enumerate(outs):
        span = out.shape[1] // 2
        for part in range(2):
            copies.append(
                pltpu.make_async_copy(
                    refs[part * n + i],
                    out.at[:, part * span : (part + 1) * span],
                    sems.at[2 * i + part],
                )
            )
            copies[-1].start()
    for copy in copies:
        copy.wait()


def hidden_kernel(pieces, *refs):
    arrived, (*wides, out_ref, x_ref, sems) = refs[:pieces], refs[pieces:]
    rows, span = arrived[0].shape[0], wides[0].shape[1] // 2
    loads = [
        pltpu.make_async_copy(a, x_ref.at[i * rows : (i + 1) * rows, :], sems.at[i])
        for i, a in enumerate(arrived)
    ]
    for load in loads:
        load.start()
    for load in loads:
        load.wait()
    x = x_ref[...]
    for i, wide in enumerate(wides):
        both = dotf(x, wide[...])
        done = jax.nn.silu(both[:, :span]) * both[:, span:]
        out_ref[:, i * span : (i + 1) * span] = done.astype(BF16)


def down_kernel(early, n, h_ref, *refs):
    parts, outs, (down_ref, sems) = refs[:n], refs[n:-2], refs[-2:]
    rows = parts[-1].shape[0]
    loads = [
        pltpu.make_async_copy(p, down_ref.at[i * rows : (i + 1) * rows, :], sems.at[i])
        for i, p in enumerate(parts[early:])
    ]
    for load in loads:
        load.start()
    at = 0
    total = None
    for part in parts[:early]:
        done = dotf(h_ref[:, at : at + part.shape[0]], part[...])
        total = done if total is None else total + done
        at += part.shape[0]
    for load in loads:
        load.wait()
    done = dotf(h_ref[:, at:], down_ref[...])
    total = done if total is None else total + done
    at = 0
    for out in outs:
        out[...] = total[at : at + out.shape[0]].astype(BF16)
        at += out.shape[0]


def body(
    mix_tokens,
    mix_gain,
    w_branch,
    w_gate_branch,
    conv_taps,
    recur_gate_w,
    inject_gate_w,
    decay_logit,
    decay_kick,
    w_mix_out,
    moe_tokens,
    moe_gain,
    expert_ids,
    route_weight,
    expert_gate_w,
    expert_up_w,
    expert_down_w,
):
    shape = jax.ShapeDtypeStruct
    me = lax.axis_index(TP)
    here = lax.axis_index(EP)
    count = lax.axis_size(TP)
    ep_size = lax.axis_size(EP)
    direct = 1 < ep_size <= 8
    place = jnp.stack([me, here, here if direct else 0 * here]).astype(jnp.int32)
    rows, width = mix_tokens.shape
    cols = w_branch.shape[1]
    taps_count = conv_taps.shape[0]
    half = max(count // 2, 1)

    lead = from_behind(mix_tokens[rows - SUB :], (EP, TP))

    local_rows, top_count = expert_ids.shape
    slots_total = 2 * local_rows * top_count
    room = slots_total // ep_size
    pieces = ep_size if direct else 1
    outgoing = call(
        functools.partial(dispatch_kernel, ep_size, room),
        tuple(shape((slots_total // pieces, width), BF16) for _ in range(pieces)),
        2 * local_rows * slots_total * width,
        place,
        moe_tokens,
        moe_gain,
        expert_ids.T,
        smem=(0,),
        alone=True,
    )
    arrived = exchange_all(outgoing)
    gate_parts = spread(expert_gate_w[0])
    up_parts = spread(expert_up_w[0])
    down = expert_down_w[0]
    first = width * SPLIT // 16 // 128 * 128
    spans = (first, width - first)
    head_count, head_dim, _ = recur_gate_w.shape
    group = 256 if cols % 256 == 0 and 256 % head_dim == 0 else cols
    gates, *down_cut = call(
        functools.partial(prepare_kernel, spans),
        (
            shape((cols // group, group, 2 * group), BF16),
            *[shape((down.shape[0], span), BF16) for span in spans],
        ),
        4 * cols * group * head_dim,
        down,
        recur_gate_w.reshape(cols, head_dim),
        inject_gate_w.reshape(cols, head_dim),
    )
    down_parts = [spread(part) for part in down_cut]

    mixer_in = call(
        norm_kernel,
        shape((rows, width), BF16),
        2 * rows * rows * width,
        mix_tokens,
        mix_gain,
        alone=True,
    )
    leads = spread(lead)
    blocks = spread(mixer_in)

    slowness = jax.nn.softplus(-decay_logit)[None, :]
    kick = call(
        kick_kernel,
        shape((count, rows, cols), F32),
        6 * count * rows * rows * head_count,
        decay_kick.T,
        stay=True,
    )
    parts = {}

    def run_blocks(ks):
        heads = call(
            lead_kernel,
            shape((len(ks), leads[0].shape[0], cols), F32),
            2 * len(ks) * leads[0].shape[0] * width * cols,
            mix_gain,
            w_branch,
            *[leads[k] for k in ks],
            stay=True,
        )
        outs = (
            shape((len(ks), 2, rows, cols), BF16),
            shape((len(ks), 3 * SUB, cols), F32),
        )
        edges = []
        if ks[-1] == count - 1:
            outs += (shape((2, cols), F32),)
            edges = [parts[g][1] for g in sorted(parts)]
        made = call(
            functools.partial(block_kernel, taps_count, count, ks, len(edges)),
            outs,
            2 * len(ks) * rows * cols * (2 * width + 2 * group),
            place,
            *edges,
            kick,
            w_branch,
            w_gate_branch,
            conv_taps,
            gates,
            slowness,
            heads,
            *[blocks[k] for k in ks],
            scratch=(
                pltpu.VMEM((rows + (taps_count - 1) * SUB, cols), F32),
                pltpu.VMEM((rows, cols), F32),
                pltpu.VMEM((rows, 2 * cols), F32),
            ),
            smem=(0,),
            stay=True,
        )
        parts[ks] = made

    run_blocks(tuple(range(half)))
    for k in range(half, count):
        run_blocks((k,))
    groups = sorted(parts)
    edges = [parts[ks][1] for ks in groups]
    totals, holds = entering(parts[groups[-1]][2])

    near_down = call(
        stack_kernel,
        shape((half * down.shape[0], spans[-1]), BF16),
        1000,
        *down_parts[-1][:half],
        scratch=(pltpu.SemaphoreType.DMA((half,)),),
        far=tuple(range(half)),
        stay=True,
    )
    pair = min(count, 2)
    wides = [w_mix_out] + [swap(w_mix_out, TP, 1)] * (pair - 1)
    wides = call(
        functools.partial(stage_kernel, pair),
        tuple(shape(w.shape, BF16) for w in wides),
        1000,
        *wides,
        scratch=(pltpu.SemaphoreType.DMA((pair,)),),
        far=tuple(range(pair)),
        stay=True,
    )
    mixed = {}
    for g in [tuple(range(half, count)), tuple(range(half))]:
        if g:
            args = [place, *totals, *edges, *[parts[p][0] for p in groups if set(p) <= set(g)]]
            made = call(
                functools.partial(mix_kernel, holds, len(groups), g),
                tuple(shape((rows, cols), BF16) for _ in g),
                2 * len(g) * rows * rows * cols,
                *args,
                scratch=(pltpu.VMEM((ep_size, 2, cols), F32),),
                smem=(0,),
                stay=True,
            )
            mixed.update(zip(g, made))
    made = {}
    for k in range(count - pair, -1, -pair):
        mine = [mixed[k]] + [swap(mixed[k + i], TP, 1) for i in range(1, pair)]
        made[k] = call(
            out_kernel,
            shape((rows, width), BF16 if k or count <= 2 else F32),
            2 * pair * rows * cols * width,
            *mine,
            *wides,
            stay=k == 0 and count > 2,
        )
    bit = pair
    while bit < count:
        for k in sorted((k for k in made if not k & bit), reverse=True):
            last = k == 0 and 2 * bit == count
            made[k] = call(
                add_kernel,
                shape((rows, width), BF16 if k or last else F32),
                rows * width,
                made[k],
                swap(made.pop(k ^ bit), TP, bit),
            )
        bit *= 2
    mixer_out = made[0]

    inner, span = gate_parts[0].shape
    staged = call(
        functools.partial(stage_pairs_kernel, count),
        tuple(shape((inner, 2 * span), BF16) for _ in range(count)),
        1000,
        *gate_parts,
        *up_parts,
        scratch=(pltpu.SemaphoreType.DMA((2 * count,)),),
        far=tuple(range(2 * count)),
        stay=True,
    )
    hidden = call(
        functools.partial(hidden_kernel, pieces),
        shape((slots_total, count * span), BF16),
        4 * count * slots_total * width * span,
        *arrived,
        *staged,
        scratch=(pltpu.VMEM((slots_total, width), BF16), pltpu.SemaphoreType.DMA((pieces,))),
        far=tuple(range(pieces)),
        stay=True,
    )
    table = call(
        functools.partial(table_kernel, ep_size, room),
        shape((3, local_rows, slots_total), BF16),
        1000,
        place,
        expert_ids,
        route_weight,
        smem=(0,),
        stay=True,
    )
    held = []
    for i, span in enumerate(spans):
        final = i == len(spans) - 1
        near = [near_down] if final else []
        far = down_parts[i][half:] if final else down_parts[i]
        done = call(
            functools.partial(down_kernel, len(near), len(near) + len(far)),
            tuple(shape((slots_total // pieces, span), BF16) for _ in range(pieces)),
            2 * slots_total * span * count * down.shape[0],
            hidden,
            *near,
            *far,
            scratch=(
                pltpu.VMEM((len(far) * down.shape[0], span), BF16),
                pltpu.SemaphoreType.DMA((len(far),)),
            ),
            far=tuple(range(1 + len(near), 1 + len(near) + len(far))),
        )
        held.append(
            call(
                functools.partial(combine_kernel, len(held) if final else 0),
                shape((local_rows, width if final else span), BF16),
                6 * local_rows * slots_total * span,
                table,
                *(held if final else []),
                *exchange_all(done),
                stay=not final,
            )
        )
    expert_out = held[-1]
    return (mixer_out, expert_out)


def solution(mesh):
    placed = (
        P((EP, TP), None),
        P(),
        P(None, TP),
        P(None, TP),
        P(None, TP),
        P(TP, None, None),
        P(TP, None, None),
        P(TP),
        P(EP, TP),
        P(TP, None),
        P((EP, TP), None),
        P(),
        P((EP, TP), None),
        P((EP, TP), None),
        P(EP, None, TP),
        P(EP, None, TP),
        P(EP, TP, None),
    )
    return jax.shard_map(
        body,
        mesh=mesh,
        in_specs=placed,
        out_specs=(P((EP, TP), None), P((EP, TP), None)),
        check_vma=False,
    )
```
